512 devices in a mesh: sp: 16 (over z), fs: 4 (over y), tp: 8 (over x, core).
Axes of the slice: x: 4, y: 4, z: 16, core: 2. Of those that a mesh axis runs over, the one named last changes fastest.
Arguments:
- tokens: bfloat16 [4, 16384, 2048], P('fs', 'sp', 'tp'), may hold values from -8 to 8
- norm_gain: float32 [2048], replicated, may hold values from 0.1 to 1.9
- w_query: bfloat16 [2048, 1024], P(('sp', 'fs'), 'tp'), may hold values from -4 to 4
- w_key: bfloat16 [2048, 512], P(('sp', 'fs'), 'tp'), may hold values from -0.16 to 0.16
- w_value: bfloat16 [2048, 512], P(('sp', 'fs'), 'tp'), may hold values from -0.125 to 0.125
- w_conv_in: bfloat16 [2048, 1024], P(('sp', 'fs'), 'tp'), may hold values from -0.125 to 0.125
- w_conv_b: bfloat16 [2048, 1024], P(('sp', 'fs'), 'tp'), may hold values from -0.125 to 0.125
- w_conv_c: bfloat16 [2048, 1024], P(('sp', 'fs'), 'tp'), may hold values from -0.125 to 0.125
- conv_taps: bfloat16 [3, 1024], P(None, 'tp'), may hold values from -3.5 to 3.5
- sink_logits: float32 [16], P('tp'), may hold values from 1 to 5
- w_attn_out: bfloat16 [1024, 2048], P('tp', ('sp', 'fs')), may hold values from -0.375 to 0.375
- w_conv_out: bfloat16 [1024, 2048], P('tp', ('sp', 'fs')), may hold values from -0.125 to 0.125
Outputs:
- mixed: bfloat16 [4, 16384, 2048], P('fs', ('sp', 'tp'))
The draws below stay inside these ranges and needn't reach their ends.
All inputs are finite; a program needn't handle non-finite values.
Results may differ from the reference program's by a relative error of at most 0.02.
Values may be sent and summed in bfloat16 or wider, within the bound.
A program may use at most 128 MiB of HBM per device.

```python
import jax
import jax.numpy as jnp
from jax import lax

D = 2048
HEADS = 16
KV_HEADS = 8
HEAD = 64
CONV = 1024
WINDOW = 128
SEQS = 4
LENGTH = 16384
N_TP = 8


def query_key_pair(key):
    folded = jax.random.fold_in(key, 11)
    first, second = jax.random.split(folded, 2)
    key_weights = jnp.clip(jax.random.normal(first, (D, KV_HEADS * HEAD), jnp.float32) * D ** (-0.5), -0.15, 0.15)
    query_weights = jax.random.normal(second, (D, HEADS * HEAD), jnp.float32) * D ** (-0.5)
    query_weights = jnp.clip(query_weights, -4.0, 4.0)
    return (query_weights, key_weights)


def draw_w_query(key, part):
    return query_key_pair(key)[0].astype(jnp.bfloat16)


def draw_w_key(key, part):
    return query_key_pair(key)[1].astype(jnp.bfloat16)


def draw_tokens(key, part):
    folded = jax.random.fold_in(key, 23)
    first = jax.random.fold_in(folded, 0)
    values = jax.random.normal(first, (SEQS, LENGTH, D), jnp.float32)
    return jnp.clip(values, -8.0, 8.0).astype(jnp.bfloat16)


def block_levels(own_key, extent, shards, least, top_value):
    def one(axis_at, shards_of):
        heights = jax.random.uniform(jax.random.fold_in(jax.random.fold_in(own_key, 6), axis_at), (shards_of,), jnp.float32, least / len(shards), top_value / len(shards))
        return jnp.repeat(jnp.exp(heights), extent[axis_at] // shards_of).reshape((-1,) + (1,) * (len(extent) - axis_at - 1))

    gain = one(*shards[0])
    for cut in shards[1:]:
        gain = gain * one(*cut)
    return gain


def normal_values(key, dims, deviation, bound, shards=(), kind=jnp.bfloat16):
    entries = jax.random.normal(key, dims, jnp.float32) * deviation
    if len(shards) > 0:
        entries = block_levels(key, dims, shards, -0.22, 0.18) * entries
    return jnp.clip(entries, min=-bound, max=bound).astype(kind)


def setup_inputs(seed: int = 0) -> dict:
    key_list = jax.random.split(jax.random.key(seed), 13)
    return {
        "tokens": draw_tokens(jax.random.fold_in(key_list[12], 71), 0),
        "norm_gain": jnp.clip(1.0 + 0.18 * jax.random.normal(key_list[1], (D,), jnp.float32), 0.1, 1.9),
        "w_query": draw_w_query(jax.random.fold_in(key_list[12], 71), 0),
        "w_key": draw_w_key(jax.random.fold_in(key_list[12], 71), 0),
        "w_value": normal_values(key_list[4], (D, KV_HEADS * HEAD), D ** -0.5, 0.125, ((0, 64), (1, 8))),
        "w_conv_in": normal_values(key_list[5], (D, CONV), D ** -0.5, 0.125, ((0, 64), (1, 8))),
        "w_conv_b": normal_values(key_list[6], (D, CONV), D ** -0.5, 0.125, ((0, 64), (1, 8))),
        "w_conv_c": normal_values(key_list[7], (D, CONV), D ** -0.5, 0.125, ((0, 64), (1, 8))),
        "conv_taps": normal_values(key_list[8], (3, CONV), 3 ** -0.5, 3.5, ((1, 8),)),
        "sink_logits": jnp.clip(1.0 + 4.0 * jax.random.uniform(key_list[9], (HEADS,), jnp.float32) ** block_levels(key_list[9], (HEADS,), ((0, 8),), -0.2, 0.2), 1.0, 5.0),
        "w_attn_out": normal_values(key_list[10], (HEADS * HEAD, D), (D // 8) ** -0.5, 0.375, ((0, 8), (1, 64))),
        "w_conv_out": normal_values(key_list[11], (CONV, D), D ** -0.5, 0.125, ((0, 8), (1, 64))),
    }


def norm_rows(tokens, norm_gain):
    values = tokens.astype(jnp.float32)
    average = lax.optimization_barrier(jnp.mean(values, axis=-1, keepdims=True))
    centred = values - average
    variance = lax.optimization_barrier(jnp.mean(centred * centred, axis=-1, keepdims=True))
    return (centred * lax.rsqrt(variance + 1e-05) * norm_gain.astype(jnp.float32)).astype(jnp.bfloat16)

def project(normed, weight):
    return jnp.dot(normed, weight, preferred_element_type=jnp.float32).astype(jnp.bfloat16)

def window_attention(queries, keys, values, sink_logits):
    length = queries.shape[0]
    blocks = length // WINDOW
    group = HEADS // KV_HEADS
    query_form = queries.astype(jnp.float32).reshape(blocks, WINDOW, KV_HEADS, group, HEAD)
    zero_rows = jnp.zeros((WINDOW, KV_HEADS * HEAD), jnp.bfloat16)
    padded_keys = jnp.concatenate([zero_rows, keys], axis=0).astype(jnp.float32).reshape(blocks + 1, WINDOW, KV_HEADS, HEAD)
    padded_values = jnp.concatenate([zero_rows, values], axis=0).astype(jnp.float32).reshape(blocks + 1, WINDOW, KV_HEADS, HEAD)
    band_keys = jnp.concatenate([padded_keys[:-1], padded_keys[1:]], axis=1)
    band_values = jnp.concatenate([padded_values[:-1], padded_values[1:]], axis=1)
    scores = jnp.einsum('bqkgd,bskd->bkgqs', query_form, band_keys) * HEAD ** (-0.5)
    row_ids = jnp.arange(WINDOW, dtype=jnp.int32)[:, None]
    col_ids = jnp.arange(2 * WINDOW, dtype=jnp.int32)[None, :]
    distance = WINDOW + row_ids - col_ids
    head_ids = jnp.arange(HEADS, dtype=jnp.int32).reshape(KV_HEADS, group)
    slopes = jnp.exp2(-8.0 * (head_ids + 1).astype(jnp.float32) / HEADS)
    scores = scores - slopes[:, :, None, None] * distance.astype(jnp.float32)
    key_place = jnp.arange(blocks, dtype=jnp.int32)[:, None] * WINDOW - WINDOW + jnp.arange(2 * WINDOW, dtype=jnp.int32)[None, :]
    inside = (distance >= 0) & (distance < WINDOW)
    keep = inside[None, None, None, :, :] & (key_place >= 0)[:, None, None, None, :]
    scores = jnp.where(keep, scores, -jnp.inf)
    sinks = sink_logits.astype(jnp.float32).reshape(KV_HEADS, group)[:, :, None, None]
    highest = jnp.maximum(lax.optimization_barrier(jnp.max(scores, axis=-1, keepdims=True)), sinks)
    raised = jnp.exp(scores - highest)
    denominator = lax.optimization_barrier(jnp.sum(raised, axis=-1, keepdims=True)) + jnp.exp(sinks - highest)
    weights = (raised / denominator).astype(jnp.bfloat16)
    mixed = jnp.einsum('bkgqs,bskd->bqkgd', weights.astype(jnp.float32), band_values)
    return mixed.astype(jnp.bfloat16).reshape(length, HEADS * HEAD)

def reference(tokens, norm_gain, w_query, w_key, w_value, w_conv_in, w_conv_b, w_conv_c, conv_taps, sink_logits, w_attn_out, w_conv_out):
    normed_all = norm_rows(tokens, norm_gain)
    head_cols = HEADS * HEAD // N_TP
    chan_cols = CONV // N_TP
    taps = conv_taps.astype(jnp.float32)

    def one_sequence(normed):
        queries = project(normed, w_query)
        keys = project(normed, w_key)
        values = project(normed, w_value)
        inner = project(normed, w_conv_in)
        gate_b = project(normed, w_conv_b)
        gate_c = project(normed, w_conv_c)
        attended = window_attention(queries, keys, values, sink_logits)
        product = (gate_c.astype(jnp.float32) * inner.astype(jnp.float32)).astype(jnp.bfloat16)
        padded = jnp.concatenate([jnp.zeros((2, CONV), jnp.float32), product.astype(jnp.float32)], axis=0)
        length = product.shape[0]
        filtered = taps[0] * padded[0:length] + taps[1] * padded[1:length + 1] + taps[2] * padded[2:length + 2]
        conv_out = (gate_b.astype(jnp.float32) * filtered).astype(jnp.bfloat16)
        summed = jnp.zeros((length, D), jnp.float32)
        for group_id in range(N_TP):
            head_slice = slice(group_id * head_cols, (group_id + 1) * head_cols)
            chan_slice = slice(group_id * chan_cols, (group_id + 1) * chan_cols)
            partial_sum = jnp.dot(attended[:, head_slice], w_attn_out[head_slice], preferred_element_type=jnp.float32)
            partial_sum = partial_sum + jnp.dot(conv_out[:, chan_slice], w_conv_out[chan_slice], preferred_element_type=jnp.float32)
            summed = summed + partial_sum.astype(jnp.bfloat16).astype(jnp.float32)
        return summed.astype(jnp.bfloat16)
    return lax.map(one_sequence, normed_all)
```

```python
import functools

import jax
import jax.numpy as jnp
from jax import lax
from jax.experimental import pallas as pl
from jax.experimental.pallas import tpu as pltpu
from jax.sharding import PartitionSpec as P

HEADS = 16
HEAD = 64
WINDOW = 128
NZ, NY, NX = 16, 4, 4
MESH = pl.DeviceIdType.MESH
NT = (((1,), (1,)), ((), ()))

STREAMS = (("zy", 256), ("zy", 384), ("zy", 384), ("yz", 256), ("yz", 384))
UP = (8, 7, 8, 7, 8)


def kernel(
    tok, gain, wq, wk, wv, wi, wb, wc, taps, sinks, wao, wco,
    out,
    T, N, B0, B1, B2, B3, B4, Q, KV, PR, GB, BIAS, AALL, AOUT, XS, XR, ACC, OUTV,
    lsem, osem, zs, zr, ys, yr, ays, ayr, xs, xr, ds, dr, oxs, oxr, hs, hr, as_, ar, es, er,
):
    z = lax.axis_index("sp")
    y = lax.axis_index("fs")
    t = lax.axis_index("tp")
    x = t // 2
    c = t % 2
    bufs = (B0, B1, B2, B3, B4)

    def dev(dz=0, dy=0, dx=0):
        return (
            lax.rem(z + NZ + dz, NZ),
            lax.rem(y + NY + dy, NY),
            lax.rem(x + NX + dx, NX) * 2 + c,
        )

    partner = (z, y, x * 2 + (1 - c))

    def rc(src, dst, ssem, rsem, to):
        return pltpu.make_async_remote_copy(
            src_ref=src, dst_ref=dst, send_sem=ssem, recv_sem=rsem, device_id=to, device_id_type=MESH
        )

    def tload(i):
        rows = pl.ds(256 * i, 256)
        return pltpu.make_async_copy(tok.at[rows, :], T.at[t, rows, :], lsem.at[i])

    for i in range(4):
        tload(i).start()

    own = pl.ds(pl.multiple_of(32 * (NY * z + y), 32), 32)
    B0[own, 0:128] = wq[...]
    B0[own, 128:256] = jnp.concatenate([wk[...], wv[...]], axis=1)
    B1[own, 0:128] = wi[...]
    B1[own, 128:256] = wb[...]
    B1[own, 256:384] = wc[...]
    B3[own, 0:128] = wao[...]
    B3[own, 128:256] = wco[...]

    barrier = pltpu.get_barrier_semaphore()
    peers = [dev(dz=1), dev(dz=-1), dev(dy=1), dev(dy=-1), dev(dx=1), dev(dx=-1), dev(dx=2), partner]
    for peer in peers:
        pl.semaphore_signal(barrier, inc=1, device_id=peer, device_id_type=MESH)
    pl.semaphore_wait(barrier, len(peers))

    def zblock(st, b):
        buf = bufs[st]
        if STREAMS[st][0] == "zy":
            return buf.at[pl.ds(pl.multiple_of(32 * (NY * b + y), 32), 32), :]
        return buf.at[pl.ds(pl.multiple_of(128 * b, 128), 128), :]

    def yblock(st, b, dy):
        yy = lax.rem(y + NY + dy, NY)
        return bufs[st].at[pl.ds(pl.multiple_of(32 * (NY * b + yy), 32), 32), :]

    def steps(st, way):
        return UP[st] if way == 0 else 15 - UP[st]

    def origin(way, s):
        return lax.rem(z + NZ - s, NZ) if way == 0 else lax.rem(z + s, NZ)

    def zcopy(st, way, s, recv):
        ref = zblock(st, origin(way, s + 1 if recv else s))
        return rc(ref, ref, zs.at[st, way, s], zr.at[st, way, s], dev(dz=1 if way == 0 else -1))

    def z_send(st, s):
        for way in (0, 1):
            if s < steps(st, way):
                zcopy(st, way, s, False).start()

    def z_wait(st, s):
        for way in (0, 1):
            if s < steps(st, way):
                zcopy(st, way, s, True).wait_recv()

    def slots(st, s):
        if s < 0:
            return [(0, 0, 0)]
        return [(1 + 8 * way + s, way, s + 1) for way in (0, 1) if s < steps(st, way)]

    def ycopy(st, slot, b, k, recv):
        if k == 2:
            fwd_up = slot < 9
            if recv:
                ref = yblock(st, b, 2)
            else:
                ref = yblock(st, b, -1 if fwd_up else 1)
            to = dev(dy=1 if fwd_up else -1)
        else:
            ref = yblock(st, b, 0 if not recv else (-1 if k == 0 else 1))
            to = dev(dy=1 if k == 0 else -1)
        return rc(ref, ref, ys.at[st, slot, k], yr.at[st, slot, k], to)

    def y_send(st, s):
        for slot, way, d in slots(st, s):
            for k in (0, 1):
                ycopy(st, slot, origin(way, d), k, False).start()

    def y_fwd(st, s):
        for slot, way, d in slots(st, s):
            b = origin(way, d)
            first = 0 if slot < 9 else 1
            ycopy(st, slot, b, first, True).wait_recv()
            ycopy(st, slot, b, 2, False).start()

    def y_fin(st, s):
        for slot, way, d in slots(st, s):
            b = origin(way, d)
            ycopy(st, slot, b, 1 if slot < 9 else 0, True).wait_recv()
            ycopy(st, slot, b, 2, True).wait_recv()

    def aycopy(st, k, recv):
        up = st % 2 == 0
        if k == 2:
            ref = yblock(st, z, 2) if recv else yblock(st, z, -1 if up else 1)
            to = dev(dy=1 if up else -1)
        else:
            ref = yblock(st, z, 0 if not recv else (-1 if k == 0 else 1))
            to = dev(dy=1 if k == 0 else -1)
        return rc(ref, ref, ays.at[st - 3, k], ayr.at[st - 3, k], to)

    def ay_send(st):
        aycopy(st, 0, False).start()
        aycopy(st, 1, False).start()

    def ay_fwd(st):
        first = 0 if st % 2 == 0 else 1
        aycopy(st, first, True).wait_recv()
        aycopy(st, 2, False).start()
        aycopy(st, 1 - first, True).wait_recv()

    def ay_fin(st):
        aycopy(st, 2, True).wait_recv()

    ox_parts = (
        (1, 0, 256, 4, 0), (2, 0, 128, 4, 256), (2, 128, 256, 2, 0), (3, 0, 256, 2, 128),
    )

    def oxcopy(k):
        d, lo, hi, st, at = ox_parts[k]
        return rc(
            B3.at[own, lo:hi], bufs[st].at[own, at : at + hi - lo], oxs.at[k], oxr.at[k], dev(dx=-d)
        )

    def tchunk(i, dx, cc):
        tt = lax.rem(x + NX + dx, NX) * 2 + cc
        return T.at[tt, pl.ds(256 * i, 256), :]

    def tcopy(i, k, recv):
        up = i % 2 == 0
        if k == 2:
            ref = tchunk(i, 2, c) if recv else tchunk(i, -1 if up else 1, c)
            to = dev(dx=1 if up else -1)
        else:
            ref = tchunk(i, 0 if not recv else (-1 if k == 0 else 1), c)
            to = dev(dx=1 if k == 0 else -1)
        return rc(ref, ref, xs.at[i, k], xr.at[i, k], to)

    def dcopy(i, k, recv):
        ref = tchunk(i, (0, -1, 1, 2)[k], c if not recv else 1 - c)
        return rc(ref, ref, ds.at[i, k], dr.at[i, k], partner)

    def t_send(i):
        tload(i).wait()
        tcopy(i, 0, False).start()
        tcopy(i, 1, False).start()
        dcopy(i, 0, False).start()

    def t_fwd(i):
        up = i % 2 == 0
        first = 0 if up else 1
        tcopy(i, first, True).wait_recv()
        tcopy(i, 2, False).start()
        dcopy(i, 1 + first, False).start()
        tcopy(i, 1 - first, True).wait_recv()
        dcopy(i, 2 - first, False).start()

    def t_fwd2(i):
        tcopy(i, 2, True).wait_recv()
        dcopy(i, 3, False).start()

    def t_fin(i):
        for k in range(4):
            dcopy(i, k, True).wait_recv()

    def norm(i):
        @pl.loop(0, 8)
        def _(j):
            rows = pl.ds(pl.multiple_of(256 * i + 32 * j, 32), 32)
            total = T[0, rows, :].astype(jnp.float32)
            for k in range(1, 8):
                total += T[k, rows, :].astype(jnp.float32)
            average = jnp.sum(total, axis=1, keepdims=True) * (1.0 / 2048)
            squares = jnp.zeros((32, 256), jnp.float32)
            for k in range(8):
                centred = T[k, rows, :].astype(jnp.float32) - average
                squares += centred * centred
            variance = jnp.sum(squares, axis=1, keepdims=True) * (1.0 / 2048)
            scale = lax.rsqrt(variance + 1e-05)
            for k in range(8):
                centred = T[k, rows, :].astype(jnp.float32) - average
                cols = slice(256 * k, 256 * k + 256)
                N[rows, cols] = (centred * scale * gain[:, cols]).astype(jnp.bfloat16)

    def project(i):
        rows = slice(256 * i, 256 * i + 256)
        normed = N[rows, :]
        qkv = jnp.dot(normed, B0[...], preferred_element_type=jnp.float32)
        Q[rows, :] = qkv[:, 0:128].astype(jnp.bfloat16)
        KV[128 + 256 * i : 128 + 256 * i + 256, :] = qkv[:, 128:256].astype(jnp.bfloat16)
        ibc = jnp.dot(normed, B1[...], preferred_element_type=jnp.float32).astype(jnp.bfloat16)
        inner = ibc[:, 0:128].astype(jnp.float32)
        gate_c = ibc[:, 256:384].astype(jnp.float32)
        product = (gate_c * inner).astype(jnp.bfloat16)
        PR[16 + 256 * i : 16 + 256 * i + 256, :] = product.astype(jnp.float32)
        GB[rows, :] = ibc[:, 128:256]

    def halo(k):
        to = dev(dz=1)
        if k == 0:
            return rc(KV.at[1024:1152, :], KV.at[0:128, :], hs.at[0], hr.at[0], to)
        return rc(PR.at[1032:1040, :], PR.at[8:16, :], hs.at[1], hr.at[1], to)

    def bias_init():
        row = lax.broadcasted_iota(jnp.int32, (128, 512), 0)
        col = lax.broadcasted_iota(jnp.int32, (128, 512), 1)
        upper = col >= 256
        distance = 128 + row - jnp.where(upper, col - 256, col)
        head = jnp.where(upper, 1, 0) + 2 * t
        slope = jnp.exp2((head + 1).astype(jnp.float32) * (-8.0 / HEADS))
        keep = (distance >= 0) & (distance < WINDOW)
        BIAS[...] = jnp.where(keep, -slope * distance.astype(jnp.float32), -jnp.inf)

    def mix(k):
        r0 = pl.multiple_of(256 * lax.rem(x + k, NX), 256)
        lane = lax.broadcasted_iota(jnp.int32, (256, 128), 1)
        low = lane < 64
        for sub in range(2):
            q0 = pl.multiple_of(r0 + 128 * sub, 128)
            q = Q[pl.ds(q0, 128), :]
            kv = KV[pl.ds(q0, 256), :].astype(jnp.float32)
            vk = pltpu.roll(kv, 64, 1)
            keys = jnp.concatenate(
                [jnp.where(low, kv, 0.0), jnp.where(low, 0.0, vk)], axis=0
            ).astype(jnp.bfloat16)
            values = jnp.concatenate(
                [jnp.where(low, vk, 0.0), jnp.where(low, 0.0, kv)], axis=0
            ).astype(jnp.bfloat16)
            scores = lax.dot_general(q, keys, NT, preferred_element_type=jnp.float32)
            scores = scores * HEAD ** (-0.5) + BIAS[...]
            if sub == 0:
                col = lax.broadcasted_iota(jnp.int32, (128, 512), 1)
                place = jnp.bitwise_and(col, 255) + (1024 * z + r0 - WINDOW)
                scores = jnp.where(place >= 0, scores, -jnp.inf)
            weights = []
            for g in range(2):
                part = scores[:, 256 * g : 256 * g + 256]
                sink = sinks[0, g]
                top = jnp.maximum(jnp.max(part, axis=1, keepdims=True), sink)
                raised = jnp.exp(part - top)
                below = jnp.sum(raised, axis=1, keepdims=True) + jnp.exp(sink - top)
                weights.append((raised * (1.0 / below)).astype(jnp.bfloat16))
            attended = jnp.dot(
                jnp.concatenate(weights, axis=1), values, preferred_element_type=jnp.float32
            )
            AOUT[k, 128 * sub : 128 * sub + 128, 0:128] = attended.astype(jnp.bfloat16)
        around = PR[pl.ds(pl.multiple_of(r0 + 8, 8), 264), :]
        tap = taps[...].astype(jnp.float32)
        filtered = (
            tap[0:1] * around[6:262] + tap[1:2] * around[7:263] + tap[2:3] * around[8:264]
        )
        gate_b = GB[pl.ds(r0, 256), :].astype(jnp.float32)
        AOUT[k, :, 128:256] = (gate_b * filtered).astype(jnp.bfloat16)

    def acopy(k, recv):
        rel = NX - k
        return rc(
            AOUT.at[k], AALL.at[rel], as_.at[k - 1], ar.at[k - 1], dev(dx=k)
        )

    def final(n, mine):
        half = c if mine else 1 - c
        rows = pl.ds(pl.multiple_of(128 * half, 128), 128)
        left = jnp.concatenate(
            [AOUT[0, rows, :], AALL[1, rows, :], AALL[2, rows, :], AALL[3, rows, :]], axis=1
        )
        cols = pl.ds(pl.multiple_of(256 * n, 256), 256)
        right = jnp.concatenate([B3[cols, :], B4[cols, :], B2[cols, :]], axis=1)
        return lax.dot_general(left, right, NT, preferred_element_type=jnp.float32)

    def excopy(n):
        return rc(XS.at[n], XR.at[n], es.at[n], er.at[n], partner)

    PROJ = (0, 1)
    OZY = 2
    OYZ = (3, 4)
    for st in PROJ:
        z_send(st, 0)
        y_send(st, -1)
    for k in range(4):
        oxcopy(k).start()
    for i in range(4):
        t_send(i)
    bias_init()

    def o_step(s):
        z_wait(OZY, s)
        z_send(OZY, s + 1)
        y_send(OZY, s)
        y_fwd(OZY, s - 1)
        if s >= 1:
            y_fin(OZY, s - 2)
        for st in OYZ:
            z_wait(st, s)
            z_send(st, s + 1)

    token_events = {
        0: [], 1: [(t_fwd, 0)], 2: [(t_fwd2, 0), (t_fwd, 1)], 3: [(t_fin, 0), (norm, 0), (t_fwd2, 1)],
        4: [(t_fwd, 2)], 5: [(t_fin, 1), (norm, 1), (t_fwd2, 2)], 6: [(t_fwd, 3), (t_fin, 2), (norm, 2)],
        7: [(t_fwd2, 3)],
    }
    for s in range(8):
        for st in PROJ:
            z_wait(st, s)
            z_send(st, s + 1)
            y_send(st, s)
        for st in PROJ:
            y_fwd(st, s - 1)
            if s >= 1:
                y_fin(st, s - 2)
        for f, i in token_events[s]:
            f(i)
        if s == 1:
            for k in range(4):
                oxcopy(k).wait_recv()
            z_send(OZY, 0)
            y_send(OZY, -1)
            for st in OYZ:
                ay_send(st)
        if s == 2:
            for st in OYZ:
                ay_fwd(st)
        if s == 4:
            for st in OYZ:
                ay_fin(st)
                z_send(st, 0)
    for st in PROJ:
        y_fwd(st, 7)
        y_fin(st, 6)
    o_step(0)
    t_fin(3)
    norm(3)
    for st in PROJ:
        y_fin(st, 7)
    project(3)
    o_step(1)
    project(0)
    halo(0).start()
    halo(1).start()
    project(1)
    o_step(2)
    project(2)
    for k in range(2):
        halo(k).wait_recv()
    PR[8:16, :] = jnp.where(z > 0, PR[8:16, :], 0.0)
    o_step(3)
    mix(2)
    mix(1)
    acopy(2, False).start()
    o_step(4)
    mix(3)
    acopy(1, False).start()
    o_step(5)
    mix(0)
    acopy(3, False).start()
    o_step(6)
    o_step(7)
    y_fwd(OZY, 7)
    y_fin(OZY, 6)
    for k in (2, 1, 3):
        acopy(k, True).wait_recv()
    y_fin(OZY, 7)

    for n in range(8):
        XS[n] = final(n, False).astype(jnp.bfloat16)
        if n >= 1:
            excopy(n - 1).start()
    for n in range(8):
        ACC[n] = final(n, True)
        if n == 0:
            excopy(7).start()
    for n in range(8):
        excopy(n).wait_recv()
        OUTV[:, 256 * n : 256 * n + 256] = (ACC[n] + XR[n].astype(jnp.float32)).astype(jnp.bfloat16)
    store = pltpu.make_async_copy(OUTV, out, osem.at[0])
    store.start()

    for st in (0, 1, 2, 3, 4):
        for s in range(8):
            for way in (0, 1):
                if s < steps(st, way):
                    zcopy(st, way, s, False).wait_send()
    for st in (0, 1, 2):
        for s in range(-1, 8):
            for slot, way, d in slots(st, s):
                for k in range(3):
                    ycopy(st, slot, origin(way, d), k, False).wait_send()
    for st in OYZ:
        for k in range(3):
            aycopy(st, k, False).wait_send()
    for k in range(4):
        oxcopy(k).wait_send()
    for i in range(4):
        for k in range(3):
            tcopy(i, k, False).wait_send()
        for k in range(4):
            dcopy(i, k, False).wait_send()
    for k in range(2):
        halo(k).wait_send()
    for k in (1, 2, 3):
        acopy(k, False).wait_send()
    for n in range(8):
        excopy(n).wait_send()
    store.wait()


def on_device(
    tokens, norm_gain, w_query, w_key, w_value, w_conv_in, w_conv_b, w_conv_c,
    conv_taps, sink_logits, w_attn_out, w_conv_out,
):
    vmem = pl.BlockSpec(memory_space=pltpu.VMEM)
    smem = pl.BlockSpec(memory_space=pltpu.SMEM)
    hbm = pl.BlockSpec(memory_space=pl.ANY)
    bf, f32 = jnp.bfloat16, jnp.float32
    dma = pltpu.SemaphoreType.DMA
    V = pltpu.VMEM
    result = pl.pallas_call(
        kernel,
        out_shape=jax.ShapeDtypeStruct((128, 2048), bf),
        in_specs=[hbm] + [vmem] * 8 + [smem] + [vmem] * 2,
        out_specs=hbm,
        scratch_shapes=[
            V((8, 1024, 256), bf), V((1024, 2048), bf),
            V((2048, 256), bf), V((2048, 384), bf), V((2048, 384), bf), V((2048, 256), bf), V((2048, 384), bf),
            V((1024, 128), bf), V((1152, 128), bf), V((1040, 128), f32), V((1024, 128), bf),
            V((128, 512), f32), V((4, 256, 256), bf), V((4, 256, 256), bf),
            V((8, 128, 256), bf), V((8, 128, 256), bf), V((8, 128, 256), f32), V((128, 2048), bf),
            dma((4,)), dma((1,)),
            dma((5, 2, 8)), dma((5, 2, 8)), dma((3, 17, 3)), dma((3, 17, 3)), dma((2, 3)), dma((2, 3)),
            dma((4, 3)), dma((4, 3)), dma((4, 4)), dma((4, 4)), dma((4,)), dma((4,)),
            dma((2,)), dma((2,)), dma((3,)), dma((3,)), dma((8,)), dma((8,)),
        ],
        compiler_params=pltpu.CompilerParams(
            collective_id=0, has_side_effects=True, vmem_limit_bytes=60 * 1024 * 1024
        ),
    )(
        tokens[0], norm_gain[None], w_query, w_key, w_value, w_conv_in, w_conv_b, w_conv_c,
        conv_taps, sink_logits[None], w_attn_out.T, w_conv_out.T,
    )
    return result[None]


def solution(mesh):
    placed = (
        P("fs", "sp", "tp"),
        P(),
        P(("sp", "fs"), "tp"),
        P(("sp", "fs"), "tp"),
        P(("sp", "fs"), "tp"),
        P(("sp", "fs"), "tp"),
        P(("sp", "fs"), "tp"),
        P(("sp", "fs"), "tp"),
        P(None, "tp"),
        P("tp"),
        P("tp", ("sp", "fs")),
        P("tp", ("sp", "fs")),
    )
    return jax.shard_map(
        on_device,
        mesh=mesh,
        in_specs=placed,
        out_specs=P("fs", ("sp", "tp"), None),
        check_vma=False,
    )
```

```python
import functools

import jax
import jax.numpy as jnp
from jax import lax
from jax.experimental import pallas as pl
from jax.experimental.pallas import tpu as pltpu
from jax.sharding import PartitionSpec as P

HEADS = 16
HEAD = 64
WINDOW = 128
NZ, NY, NX = 16, 4, 4
MESH = pl.DeviceIdType.MESH
NT = (((1,), (1,)), ((), ()))

STREAMS = (("zy", 256), ("zy", 384), ("zy", 256), ("yz", 256), ("yz", 512))
UP = (8, 7, 8, 7, 8)
SKIP = ((6, 2), (6, 2), (6, 2), (6, 2), (6, 2))
DIRECT = 7
LATE = 96


def kernel(
    tok, gain, wq, wk, wv, wi, wb, wc, taps, sinks, wao, wco,
    out,
    T, N, B0, B1, B2, B3, B4, Q, KV, PR, GB, BIAS, AALL, AOUT, RLY, XS, XR, ACC, OUTV,
    lsem, osem, ss, zr, yr, ayr, tsem, xr, dr, oxr, xlr, hsem, hr, asem, ar, rr, es, er,
):
    z = lax.axis_index("sp")
    y = lax.axis_index("fs")
    t = lax.axis_index("tp")
    x = t // 2
    c = t % 2
    bufs = (B0, B1, B2, B3, B4)

    def dev(dz=0, dy=0, dx=0):
        return (
            lax.rem(z + NZ + dz, NZ),
            lax.rem(y + NY + dy, NY),
            lax.rem(x + NX + dx, NX) * 2 + c,
        )

    partner = (z, y, x * 2 + (1 - c))

    def rc(src, dst, ssem, rsem, to):
        return pltpu.make_async_remote_copy(
            src_ref=src, dst_ref=dst, send_sem=ssem, recv_sem=rsem, device_id=to, device_id_type=MESH
        )

    barrier = pltpu.get_barrier_semaphore()
    peers = [dev(dz=1), dev(dz=-1), dev(dy=1), dev(dy=-1), dev(dx=1), dev(dx=-1), dev(dx=2), partner]
    for peer in peers:
        pl.semaphore_signal(barrier, inc=1, device_id=peer, device_id_type=MESH)

    def tload(i):
        rows = pl.ds(256 * i, 256)
        return pltpu.make_async_copy(tok.at[rows, :], T.at[t, rows, :], lsem.at[i])

    for i in range(4):
        tload(i).start()

    own = pl.ds(pl.multiple_of(32 * (NY * z + y), 32), 32)
    B0[own, 0:128] = wq[...]
    B0[own, 128:256] = jnp.concatenate([wk[...], wv[...]], axis=1)
    B1[own, 0:128] = wi[...]
    B1[own, 128:256] = wb[...]
    B1[own, 256:384] = wc[...]
    B3[own, 0:128] = wao[...]
    B3[own, 128:256] = wco[...]

    pl.semaphore_wait(barrier, len(peers))

    def zblock(st, b):
        buf = bufs[st]
        if STREAMS[st][0] == "zy":
            return buf.at[pl.ds(pl.multiple_of(32 * (NY * b + y), 32), 32), :]
        if st == 4:
            return buf.at[pl.ds(pl.multiple_of(128 * b + LATE, 32), 128 - LATE), :]
        return buf.at[pl.ds(pl.multiple_of(128 * b, 128), 128), :]

    def yblock(st, b, dy):
        yy = lax.rem(y + NY + dy, NY)
        return bufs[st].at[pl.ds(pl.multiple_of(32 * (NY * b + yy), 32), 32), :]

    def steps(st, way):
        return UP[st] if way == 0 else 15 - UP[st]

    def origin(way, s):
        return lax.rem(z + NZ - s, NZ) if way == 0 else lax.rem(z + s, NZ)

    def zarrived(st, way, d):
        ref = zblock(st, origin(way, d))
        return rc(ref, ref, ss.at[st], zr.at[st, way, d - 1], dev(dz=1))

    def zpass(st, d):
        near, jump = SKIP[st]
        for way in (0, 1):
            last = steps(st, way)
            ref = zblock(st, origin(way, d))
            for hops in (1, jump):
                to = d + hops
                if hops == 1 and to > min(near, last) or hops > 1 and (d == 0 or not near < to <= last):
                    continue
                if d <= last:
                    rc(
                        ref, ref, ss.at[st], zr.at[st, way, to - 1], dev(dz=hops if way == 0 else -hops)
                    ).start()

    def zs(st):
        zpass(st, 0)

    def zv(st, d):
        for way in (0, 1):
            if d <= steps(st, way):
                zarrived(st, way, d).wait_recv()
        zpass(st, d)
        if st == 3:
            xl_send(d - 1)

    def slots(st, s):
        if s < 0:
            return [(0, 0, 0)]
        return [(1 + 8 * way + s, way, s + 1) for way in (0, 1) if s < steps(st, way)]

    def ycopy(st, slot, b, d, k, recv):
        if k == 2 and d >= DIRECT:
            ref = yblock(st, b, 2 if recv else 0)
            to = dev(dy=2)
        elif k == 2:
            fwd_up = slot < 9
            if recv:
                ref = yblock(st, b, 2)
            else:
                ref = yblock(st, b, -1 if fwd_up else 1)
            to = dev(dy=1 if fwd_up else -1)
        else:
            ref = yblock(st, b, 0 if not recv else (-1 if k == 0 else 1))
            to = dev(dy=1 if k == 0 else -1)
        return rc(ref, ref, ss.at[st], yr.at[st, slot, k], to)

    def ys(st, e):
        for slot, way, d in slots(st, e - 1):
            for k in (0, 1, 2) if e >= DIRECT else (0, 1):
                ycopy(st, slot, origin(way, d), d, k, False).start()

    def yf(st, e):
        for slot, way, d in slots(st, e - 1):
            b = origin(way, d)
            ycopy(st, slot, b, d, 0 if slot < 9 else 1, True).wait_recv()
            ycopy(st, slot, b, d, 2, False).start()

    def yn(st, e):
        for slot, way, d in slots(st, e - 1):
            b = origin(way, d)
            ycopy(st, slot, b, d, 1 if slot < 9 else 0, True).wait_recv()
            ycopy(st, slot, b, d, 2, True).wait_recv()
            if e >= DIRECT:
                ycopy(st, slot, b, d, 0 if slot < 9 else 1, True).wait_recv()

    def aycopy(st, k, recv):
        up = st % 2 == 0
        if k == 2:
            ref = yblock(st, z, 2) if recv else yblock(st, z, -1 if up else 1)
            to = dev(dy=1 if up else -1)
        else:
            ref = yblock(st, z, 0 if not recv else (-1 if k == 0 else 1))
            to = dev(dy=1 if k == 0 else -1)
        return rc(ref, ref, ss.at[st], ayr.at[st - 3, k], to)

    def ay(st):
        aycopy(st, 0, False).start()
        aycopy(st, 1, False).start()

    def ayf(st):
        aycopy(st, 0 if st % 2 == 0 else 1, True).wait_recv()
        aycopy(st, 2, False).start()

    def aye(st):
        aycopy(st, 1 if st % 2 == 0 else 0, True).wait_recv()
        aycopy(st, 2, True).wait_recv()
        zs(st)

    ox_parts = ((1, 4, 0), (2, 2, 0), (3, 4, 256))

    def oxcopy(k):
        d, st, at = ox_parts[k]
        return rc(B3.at[own, :], bufs[st].at[own, at : at + 256], ss.at[5], oxr.at[k], dev(dx=-d))

    def xlcopy(s, way, k):
        rows = pl.ds(pl.multiple_of(128 * origin(way, s + 1), 128), LATE)
        at = 256 * k
        return rc(
            B3.at[rows, :], B4.at[rows, at : at + 256], ss.at[5 + k], xlr.at[k, way, s], dev(dx=-1 if k == 0 else 1)
        )

    def xl_send(s):
        for way in (0, 1):
            if s < steps(3, way):
                for k in (0, 1):
                    xlcopy(s, way, k).start()

    def xl_wait(s):
        for way in (0, 1):
            if s < steps(3, way):
                for k in (0, 1):
                    xlcopy(s, way, k).wait_recv()

    def tchunk(i, dx, cc):
        tt = lax.rem(x + NX + dx, NX) * 2 + cc
        return T.at[tt, pl.ds(256 * i, 256), :]

    def tcopy(i, k, recv):
        up = i % 2 == 0
        if k == 2:
            ref = tchunk(i, 2, c) if recv else tchunk(i, -1 if up else 1, c)
            to = dev(dx=1 if up else -1)
        else:
            ref = tchunk(i, 0 if not recv else (-1 if k == 0 else 1), c)
            to = dev(dx=1 if k == 0 else -1)
        return rc(ref, ref, tsem.at[0], xr.at[i, k], to)

    def dcopy(i, k, recv):
        ref = tchunk(i, (0, -1, 1, 2)[k], c if not recv else 1 - c)
        return rc(ref, ref, tsem.at[0], dr.at[i, k], partner)

    def ts(i):
        tload(i).wait()
        tcopy(i, 0, False).start()
        tcopy(i, 1, False).start()
        dcopy(i, 0, False).start()

    def tf(i):
        first = i % 2
        tcopy(i, first, True).wait_recv()
        tcopy(i, 2, False).start()
        dcopy(i, 1 + first, False).start()

    def tg(i):
        first = i % 2
        tcopy(i, 1 - first, True).wait_recv()
        dcopy(i, 2 - first, False).start()

    def th(i):
        tcopy(i, 2, True).wait_recv()
        dcopy(i, 3, False).start()

    def td(i):
        for k in range(4):
            dcopy(i, k, True).wait_recv()

    def norm(i, h):
        base = 256 * i + 64 * h

        @pl.loop(0, 2)
        def _(j):
            rows = [pl.ds(pl.multiple_of(base + 32 * j + 16 * g, 16), 16) for g in range(2)]
            averages, scales = [], []
            for r in rows:
                total = T[0, r, :].astype(jnp.float32)
                for k in range(1, 8):
                    total += T[k, r, :].astype(jnp.float32)
                averages.append(jnp.sum(total, axis=1, keepdims=True) * (1.0 / 2048))
            for r, average in zip(rows, averages):
                squares = None
                for k in range(8):
                    centred = T[k, r, :].astype(jnp.float32) - average
                    squares = centred * centred if k == 0 else squares + centred * centred
                variance = jnp.sum(squares, axis=1, keepdims=True) * (1.0 / 2048)
                scales.append(lax.rsqrt(variance + 1e-05))
            for k in range(8):
                cols = slice(256 * k, 256 * k + 256)
                for r, average, scale in zip(rows, averages, scales):
                    centred = T[k, r, :].astype(jnp.float32) - average
                    N[r, cols] = (centred * scale * gain[:, cols]).astype(jnp.bfloat16)

    def proj(i):
        rows = slice(256 * i, 256 * i + 256)
        normed = N[rows, :]
        qkv = jnp.dot(normed, B0[...], preferred_element_type=jnp.float32)
        Q[rows, :] = qkv[:, 0:128].astype(jnp.bfloat16)
        KV[128 + 256 * i : 128 + 256 * i + 256, :] = qkv[:, 128:256].astype(jnp.bfloat16)
        ibc = jnp.dot(normed, B1[...], preferred_element_type=jnp.float32).astype(jnp.bfloat16)
        inner = ibc[:, 0:128].astype(jnp.float32)
        gate_c = ibc[:, 256:384].astype(jnp.float32)
        product = (gate_c * inner).astype(jnp.bfloat16)
        PR[16 + 256 * i : 16 + 256 * i + 256, :] = product.astype(jnp.float32)
        GB[rows, :] = ibc[:, 128:256]

    def halo(k):
        to = dev(dz=1)
        if k == 0:
            return rc(KV.at[1024:1152, :], KV.at[0:128, :], hsem.at[0], hr.at[0], to)
        return rc(PR.at[1032:1040, :], PR.at[8:16, :], hsem.at[1], hr.at[1], to)

    def bias_init():
        row = lax.broadcasted_iota(jnp.int32, (128, 512), 0)
        col = lax.broadcasted_iota(jnp.int32, (128, 512), 1)
        upper = col >= 256
        distance = 128 + row - jnp.where(upper, col - 256, col)
        head = jnp.where(upper, 1, 0) + 2 * t
        slope = jnp.exp2((head + 1).astype(jnp.float32) * (-8.0 / HEADS))
        keep = (distance >= 0) & (distance < WINDOW)
        BIAS[...] = jnp.where(keep, -slope * distance.astype(jnp.float32), -jnp.inf)

    def mix(k, u):
        q0 = pl.multiple_of(256 * lax.rem(x + k, NX) + 128 * u, 128)
        lane = lax.broadcasted_iota(jnp.int32, (256, 128), 1)
        low = lane < 64
        q = Q[pl.ds(q0, 128), :]
        kv = KV[pl.ds(q0, 256), :].astype(jnp.float32)
        vk = pltpu.roll(kv, 64, 1)
        keys = jnp.concatenate(
            [jnp.where(low, kv, 0.0), jnp.where(low, 0.0, vk)], axis=0
        ).astype(jnp.bfloat16)
        values = jnp.concatenate(
            [jnp.where(low, vk, 0.0), jnp.where(low, 0.0, kv)], axis=0
        ).astype(jnp.bfloat16)
        scores = lax.dot_general(q, keys, NT, preferred_element_type=jnp.float32)
        scores = scores * HEAD ** (-0.5) + BIAS[...]
        if u == 0:
            col = lax.broadcasted_iota(jnp.int32, (128, 512), 1)
            place = jnp.bitwise_and(col, 255) + (1024 * z + q0 - WINDOW)
            scores = jnp.where(place >= 0, scores, -jnp.inf)
        weights = []
        for g in range(2):
            part = scores[:, 256 * g : 256 * g + 256]
            sink = sinks[0, g]
            top = jnp.maximum(jnp.max(part, axis=1, keepdims=True), sink)
            raised = jnp.exp(part - top)
            below = jnp.sum(raised, axis=1, keepdims=True) + jnp.exp(sink - top)
            weights.append((raised * (1.0 / below)).astype(jnp.bfloat16))
        attended = jnp.dot(
            jnp.concatenate(weights, axis=1), values, preferred_element_type=jnp.float32
        )
        half = slice(128 * u, 128 * u + 128)
        AOUT[k, half, 0:128] = attended.astype(jnp.bfloat16)
        around = PR[pl.ds(pl.multiple_of(q0 + 8, 8), 136), :]
        tap = taps[...].astype(jnp.float32)
        filtered = (
            tap[0:1] * around[6:134] + tap[1:2] * around[7:135] + tap[2:3] * around[8:136]
        )
        gate_b = GB[pl.ds(q0, 128), :].astype(jnp.float32)
        AOUT[k, half, 128:256] = (gate_b * filtered).astype(jnp.bfloat16)

    def acopy(k, u):
        half = pl.ds(128 * u, 128)
        if k == 2:
            return rc(AOUT.at[k, half, :], RLY.at[u], asem.at[0], rr.at[u], dev(dx=1 - 2 * u))
        return rc(AOUT.at[k, half, :], AALL.at[NX - k, half, :], asem.at[0], ar.at[k - 1, u], dev(dx=k))

    def relay(u):
        half = pl.ds(128 * u, 128)
        return rc(RLY.at[u], AALL.at[2, half, :], asem.at[1], ar.at[1, u], dev(dx=1 - 2 * u))

    def out_dot(left, buf, n, at):
        right = buf[512 * n : 512 * n + 512, at : at + 256]
        return lax.dot_general(left, right, NT, preferred_element_type=jnp.float32)

    def excopy(n):
        return rc(XS.at[n], XR.at[n], es.at[0], er.at[n], partner)

    def store(n):
        cols = slice(512 * n, 512 * n + 512)
        return pltpu.make_async_copy(OUTV.at[:, cols], out.at[:, cols], osem.at[n])

    def start():
        bias_init()

    def ox():
        for k in range(3):
            oxcopy(k).start()

    def oxw():
        for k in range(3):
            oxcopy(k).wait_recv()

    def xw(d):
        xl_wait(d - 1)

    def hs():
        halo(0).start()
        halo(1).start()

    def hw():
        halo(0).wait_recv()
        halo(1).wait_recv()
        PR[8:16, :] = jnp.where(z > 0, PR[8:16, :], 0.0)

    def asend(k, u):
        acopy(k, u).start()

    def af(u):
        acopy(2, u).wait_recv()
        relay(u).start()

    def aw(k):
        for u in (0, 1):
            (relay(u) if k == 2 else acopy(k, u)).wait_recv()

    def f0():
        for n in range(4):
            ACC[:, 512 * n : 512 * n + 512] = out_dot(AOUT[0], B3, n, 0)

    def f1():
        for n in range(4):
            ACC[:, 512 * n : 512 * n + 512] += out_dot(AALL[1], B4, n, 0)

    def f3():
        for n in range(4):
            ACC[:, 512 * n : 512 * n + 512] += out_dot(AALL[3], B4, n, 256)

    def ft():
        rows = pl.ds(pl.multiple_of(128 * (1 - c), 128), 128)
        for n in range(4):
            total = ACC[rows, 512 * n : 512 * n + 512] + out_dot(AALL[2, rows, :], B2, n, 0)
            XS[n] = total.astype(jnp.bfloat16)
            if n >= 1:
                excopy(n - 1).start()

    def fo():
        rows = pl.ds(pl.multiple_of(128 * c, 128), 128)
        for n in range(4):
            cols = slice(512 * n, 512 * n + 512)
            ACC[rows, cols] += out_dot(AALL[2, rows, :], B2, n, 0)
            if n == 0:
                excopy(3).start()

    def comb():
        rows = pl.ds(pl.multiple_of(128 * c, 128), 128)
        for n in range(4):
            cols = slice(512 * n, 512 * n + 512)
            excopy(n).wait_recv()
            OUTV[:, cols] = (ACC[rows, cols] + XR[n].astype(jnp.float32)).astype(jnp.bfloat16)
            if n >= 1:
                store(n - 1).start()

    order = (
        (start,), (zs, 1), (zs, 0), (ox,), (ay, 3), (ys, 0, 0), (ys, 1, 0), (ts, 3), (ts, 0), (ts, 2), (ts, 1),
        (ayf, 3), (zv, 1, 1), (ys, 1, 1), (yf, 0, 0), (zv, 0, 1), (ys, 0, 1), (yf, 1, 0), (oxw,), (ay, 4), (tg, 3),
        (aye, 3), (zv, 1, 2), (ys, 1, 2), (tf, 3), (zv, 0, 2), (ys, 0, 2), (yf, 1, 1), (yn, 0, 0), (yf, 0, 1),
        (yn, 1, 0), (tf, 0), (ayf, 4), (tg, 0), (yf, 1, 2), (zv, 3, 1), (zv, 1, 3), (ys, 1, 3), (yf, 0, 2),
        (zv, 0, 3), (zs, 2), (ys, 0, 3), (ys, 2, 0), (tf, 2), (yn, 1, 1), (yn, 0, 1), (tg, 2), (aye, 4), (yn, 1, 2),
        (zv, 3, 2), (tg, 1), (yf, 1, 3), (zv, 1, 4), (ys, 1, 4), (yn, 0, 2), (tf, 1), (zv, 0, 4), (ys, 0, 4),
        (yf, 0, 3), (yf, 2, 0), (zv, 4, 1), (th, 0), (yn, 1, 3), (th, 3), (zv, 3, 3), (td, 0), (yf, 1, 4),
        (norm, 0, 0), (zv, 1, 5), (ys, 1, 5), (norm, 0, 2), (zv, 0, 5), (zv, 2, 1), (ys, 0, 5), (ys, 2, 1),
        (norm, 0, 1), (yf, 0, 4), (td, 3), (norm, 3, 0), (yn, 0, 3), (norm, 3, 2), (zv, 4, 2), (xw, 1), (norm, 3, 1),
        (yn, 2, 0), (norm, 3, 3), (norm, 0, 3), (yn, 1, 4), (th, 2), (zv, 3, 4), (zv, 1, 6), (ys, 1, 6), (yf, 1, 5),
        (td, 2), (norm, 2, 0), (yf, 0, 5), (norm, 2, 2), (norm, 2, 1), (xw, 2), (zv, 0, 6), (ys, 0, 6), (yf, 2, 1),
        (norm, 2, 3), (zv, 1, 7), (ys, 1, 7), (yn, 0, 4), (th, 1), (zv, 0, 7), (zv, 2, 2), (ys, 0, 7), (ys, 2, 2),
        (zv, 4, 3), (td, 1), (norm, 1, 2), (norm, 1, 1), (yf, 1, 6), (norm, 1, 3), (xw, 3), (norm, 1, 0), (yn, 1, 5),
        (zv, 3, 5), (yn, 0, 5), (yf, 0, 6), (yn, 2, 1), (zv, 0, 8), (ys, 0, 8), (zv, 2, 3), (ys, 2, 3), (zv, 1, 8),
        (ys, 1, 8), (xw, 4), (zv, 4, 4), (yn, 1, 7), (zv, 3, 6), (xw, 5), (yn, 0, 7), (yf, 2, 2), (yn, 1, 6),
        (yn, 0, 6), (zv, 3, 7), (zv, 2, 4), (ys, 2, 4), (yf, 2, 3), (yn, 0, 8), (zv, 4, 5), (xw, 6), (yn, 2, 2),
        (yn, 1, 8), (proj, 3), (hs,), (proj, 1), (zv, 3, 8), (zv, 2, 5), (yf, 2, 4), (ys, 2, 5), (yn, 2, 3),
        (proj, 0), (zv, 4, 6), (proj, 2), (xw, 7), (zv, 4, 7), (hw,), (mix, 2, 1), (asend, 2, 1), (mix, 2, 0),
        (zv, 2, 6), (ys, 2, 6), (asend, 2, 0), (yn, 2, 4), (mix, 1, 0), (yf, 2, 5), (asend, 1, 0), (mix, 1, 1),
        (zv, 2, 7), (ys, 2, 7), (asend, 1, 1), (mix, 3, 1), (asend, 3, 1), (mix, 3, 0), (asend, 3, 0), (mix, 0, 1),
        (zv, 4, 8), (mix, 0, 0), (xw, 8), (f0,), (yf, 2, 6), (af, 1), (yn, 2, 5), (zv, 2, 8), (ys, 2, 8), (af, 0),
        (yn, 2, 7), (yn, 2, 6), (aw, 1), (aw, 3), (f1,), (f3,), (yn, 2, 8), (aw, 2), (ft,), (fo,), (comb,),
    )
    for event, *where in order:
        with jax.named_scope(event.__name__ + "_".join(map(str, where))):
            event(*where)
    store(3).start()

    def sent(ref, sem):
        pltpu.make_async_copy(ref, ref, sem).wait()

    for st in (0, 1, 2):
        sent(bufs[st].at[0:2016, :], ss.at[st])
    sent(B3.at[0:2016, :], ss.at[3])
    sent(B4.at[0 : 96 + 15 * (128 - LATE), :], ss.at[4])
    sent(B3.at[0 : 96 + 15 * LATE, :], ss.at[5])
    sent(B3.at[0 : 15 * LATE, :], ss.at[6])
    sent(T.at[0:7], tsem.at[0])
    for k in range(2):
        halo(k).wait_send()
    sent(AOUT.at[0:3], asem.at[0])
    sent(RLY, asem.at[1])
    sent(XS, es.at[0])
    for n in range(4):
        store(n).wait()


def on_device(
    tokens, norm_gain, w_query, w_key, w_value, w_conv_in, w_conv_b, w_conv_c,
    conv_taps, sink_logits, w_attn_out, w_conv_out,
):
    vmem = pl.BlockSpec(memory_space=pltpu.VMEM)
    smem = pl.BlockSpec(memory_space=pltpu.SMEM)
    hbm = pl.BlockSpec(memory_space=pl.ANY)
    bf, f32 = jnp.bfloat16, jnp.float32
    dma = pltpu.SemaphoreType.DMA
    V = pltpu.VMEM
    result = pl.pallas_call(
        kernel,
        out_shape=jax.ShapeDtypeStruct((128, 2048), bf),
        in_specs=[hbm] + [vmem] * 8 + [smem] + [vmem] * 2,
        out_specs=hbm,
        scratch_shapes=[
            V((8, 1024, 256), bf), V((1024, 2048), bf),
            V((2048, 256), bf), V((2048, 384), bf), V((2048, 256), bf), V((2048, 256), bf), V((2048, 512), bf),
            V((1024, 128), bf), V((1152, 128), bf), V((1040, 128), f32), V((1024, 128), bf),
            V((128, 512), f32), V((4, 256, 256), bf), V((4, 256, 256), bf), V((2, 128, 256), bf),
            V((4, 128, 512), bf), V((4, 128, 512), bf), V((256, 2048), f32), V((128, 2048), bf),
            dma((4,)), dma((4,)),
            dma((7,)), dma((5, 2, 8)), dma((3, 17, 3)), dma((2, 3)),
            dma((1,)), dma((4, 3)), dma((4, 4)), dma((3,)), dma((2, 2, 8)),
            dma((2,)), dma((2,)), dma((2,)), dma((3, 2)), dma((2,)), dma((1,)), dma((4,)),
        ],
        compiler_params=pltpu.CompilerParams(
            collective_id=0, has_side_effects=True, vmem_limit_bytes=60 * 1024 * 1024
        ),
    )(
        tokens[0], norm_gain[None], w_query, w_key, w_value, w_conv_in, w_conv_b, w_conv_c,
        conv_taps, sink_logits[None], w_attn_out.T, w_conv_out.T,
    )
    return result[None]


def solution(mesh):
    placed = (
        P("fs", "sp", "tp"),
        P(),
        P(("sp", "fs"), "tp"),
        P(("sp", "fs"), "tp"),
        P(("sp", "fs"), "tp"),
        P(("sp", "fs"), "tp"),
        P(("sp", "fs"), "tp"),
        P(("sp", "fs"), "tp"),
        P(None, "tp"),
        P("tp"),
        P("tp", ("sp", "fs")),
        P("tp", ("sp", "fs")),
    )
    return jax.shard_map(
        on_device,
        mesh=mesh,
        in_specs=placed,
        out_specs=P("fs", ("sp", "tp"), None),
        check_vma=False,
    )
```

```python
import functools

import jax
import jax.numpy as jnp
from jax import lax
from jax.experimental import pallas as pl
from jax.experimental.pallas import tpu as pltpu
from jax.sharding import PartitionSpec as P

HEADS = 16
HEAD = 64
WINDOW = 128
NZ, NY, NX = 16, 4, 4
MESH = pl.DeviceIdType.MESH
NT = (((1,), (1,)), ((), ()))

STREAMS = (("zy", 256), ("zy", 384), ("zy", 256), ("yz", 256), ("yz", 512))
UP = (8, 7, 8, 7, 8)
SKIP = ((6, 2), (6, 2), (6, 2), (6, 2), (6, 2))
DIRECT = 7
LATE = 96
EARLY = 4


def kernel(
    tok, gain, wq, wk, wv, wi, wb, wc, taps, sinks, wao, wco,
    out,
    T, N, B0, B1, B2, B3, B4, Q, KV, PR, GB, BIAS, AALL, AOUT, RLY, XS, XR, ACC, OUTV, PACC,
    lsem, osem, ss, zr, yr, ayr, tsem, xr, dr, oxr, xlr, hsem, hr, asem, ar, rr, es, er,
):
    z = lax.axis_index("sp")
    y = lax.axis_index("fs")
    t = lax.axis_index("tp")
    x = t // 2
    c = t % 2
    bufs = (B0, B1, B2, B3, B4)

    def dev(dz=0, dy=0, dx=0):
        return (
            lax.rem(z + NZ + dz, NZ),
            lax.rem(y + NY + dy, NY),
            lax.rem(x + NX + dx, NX) * 2 + c,
        )

    partner = (z, y, x * 2 + (1 - c))

    def rc(src, dst, ssem, rsem, to):
        return pltpu.make_async_remote_copy(
            src_ref=src, dst_ref=dst, send_sem=ssem, recv_sem=rsem, device_id=to, device_id_type=MESH
        )

    barrier = pltpu.get_barrier_semaphore()
    peers = [dev(dz=1), dev(dz=-1), dev(dy=1), dev(dy=-1), dev(dx=1), dev(dx=-1), dev(dx=2), partner]
    for peer in peers:
        pl.semaphore_signal(barrier, inc=1, device_id=peer, device_id_type=MESH)

    def tload(i):
        rows = pl.ds(256 * i, 256)
        return pltpu.make_async_copy(tok.at[rows, :], T.at[t, rows, :], lsem.at[i])

    for i in range(4):
        with jax.named_scope("load"):
            tload(i).start()

    own = pl.ds(pl.multiple_of(32 * (NY * z + y), 32), 32)
    B0[own, 0:128] = wq[...]
    B0[own, 128:256] = jnp.concatenate([wk[...], wv[...]], axis=1)
    B1[own, 0:128] = wi[...]
    B1[own, 128:256] = wb[...]
    B1[own, 256:384] = wc[...]
    B3[own, 0:128] = wao[...]
    B3[own, 128:256] = wco[...]

    with jax.named_scope("barrier"):
        pl.semaphore_wait(barrier, len(peers))

    def zblock(st, b):
        buf = bufs[st]
        if STREAMS[st][0] == "zy":
            return buf.at[pl.ds(pl.multiple_of(32 * (NY * b + y), 32), 32), :]
        if st == 4:
            return buf.at[pl.ds(pl.multiple_of(128 * b + LATE, 16), 128 - LATE), :]
        return buf.at[pl.ds(pl.multiple_of(128 * b, 128), 128), :]

    def yblock(st, b, dy):
        yy = lax.rem(y + NY + dy, NY)
        return bufs[st].at[pl.ds(pl.multiple_of(32 * (NY * b + yy), 32), 32), :]

    def steps(st, way):
        return UP[st] if way == 0 else 15 - UP[st]

    def origin(way, s):
        return lax.rem(z + NZ - s, NZ) if way == 0 else lax.rem(z + s, NZ)

    def zarrived(st, way, d):
        ref = zblock(st, origin(way, d))
        return rc(ref, ref, ss.at[st], zr.at[st, way, d - 1], dev(dz=1))

    def zpass(st, d):
        near, jump = SKIP[st]
        for way in (0, 1):
            last = steps(st, way)
            ref = zblock(st, origin(way, d))
            for hops in (1, jump):
                to = d + hops
                if hops == 1 and to > min(near, last) or hops > 1 and (d == 0 or not near < to <= last):
                    continue
                if d <= last:
                    rc(
                        ref, ref, ss.at[st], zr.at[st, way, to - 1], dev(dz=hops if way == 0 else -hops)
                    ).start()

    def zs(st):
        zpass(st, 0)

    def zv(st, d):
        for way in (0, 1):
            if d <= steps(st, way):
                zarrived(st, way, d).wait_recv()
        zpass(st, d)
        if st == 3:
            xl_send(d - 1)

    def slots(st, s):
        if s < 0:
            return [(0, 0, 0)]
        return [(1 + 8 * way + s, way, s + 1) for way in (0, 1) if s < steps(st, way)]

    def ycopy(st, slot, b, d, k, recv):
        if k == 2 and d >= DIRECT:
            ref = yblock(st, b, 2 if recv else 0)
            to = dev(dy=2)
        elif k == 2:
            fwd_up = slot < 9
            if recv:
                ref = yblock(st, b, 2)
            else:
                ref = yblock(st, b, -1 if fwd_up else 1)
            to = dev(dy=1 if fwd_up else -1)
        else:
            ref = yblock(st, b, 0 if not recv else (-1 if k == 0 else 1))
            to = dev(dy=1 if k == 0 else -1)
        return rc(ref, ref, ss.at[st], yr.at[st, slot, k], to)

    def ys(st, e):
        for slot, way, d in slots(st, e - 1):
            for k in (0, 1, 2) if e >= DIRECT else (0, 1):
                ycopy(st, slot, origin(way, d), d, k, False).start()

    def yf(st, e):
        for slot, way, d in slots(st, e - 1):
            b = origin(way, d)
            ycopy(st, slot, b, d, 0 if slot < 9 else 1, True).wait_recv()
            ycopy(st, slot, b, d, 2, False).start()

    def yn(st, e):
        for slot, way, d in slots(st, e - 1):
            b = origin(way, d)
            ycopy(st, slot, b, d, 1 if slot < 9 else 0, True).wait_recv()
            ycopy(st, slot, b, d, 2, True).wait_recv()
            if e >= DIRECT:
                ycopy(st, slot, b, d, 0 if slot < 9 else 1, True).wait_recv()

    def aycopy(st, k, recv):
        up = st % 2 == 0
        if k == 2:
            ref = yblock(st, z, 2) if recv else yblock(st, z, -1 if up else 1)
            to = dev(dy=1 if up else -1)
        else:
            ref = yblock(st, z, 0 if not recv else (-1 if k == 0 else 1))
            to = dev(dy=1 if k == 0 else -1)
        return rc(ref, ref, ss.at[st], ayr.at[st - 3, k], to)

    def ay(st):
        aycopy(st, 0, False).start()
        aycopy(st, 1, False).start()

    def ayf(st):
        aycopy(st, 0 if st % 2 == 0 else 1, True).wait_recv()
        aycopy(st, 2, False).start()

    def aye(st):
        aycopy(st, 1 if st % 2 == 0 else 0, True).wait_recv()
        aycopy(st, 2, True).wait_recv()
        zs(st)

    ox_parts = ((1, 4, 0), (2, 2, 0), (3, 4, 256))

    def oxcopy(k):
        d, st, at = ox_parts[k]
        return rc(B3.at[own, :], bufs[st].at[own, at : at + 256], ss.at[5], oxr.at[k], dev(dx=-d))

    def xlcopy(s, way, k):
        rows = pl.ds(pl.multiple_of(128 * origin(way, s + 1), 128), LATE)
        at = 256 * k
        return rc(
            B3.at[rows, :], B4.at[rows, at : at + 256], ss.at[5 + k], xlr.at[k, way, s], dev(dx=-1 if k == 0 else 1)
        )

    def xl_send(s):
        for way in (0, 1):
            if s < steps(3, way):
                for k in (0, 1):
                    xlcopy(s, way, k).start()

    def xl_wait(s):
        for way in (0, 1):
            if s < steps(3, way):
                for k in (0, 1):
                    xlcopy(s, way, k).wait_recv()

    def tchunk(i, dx, cc):
        tt = lax.rem(x + NX + dx, NX) * 2 + cc
        return T.at[tt, pl.ds(256 * i, 256), :]

    def tcopy(i, k, recv):
        up = i % 2 == 0
        if k == 2:
            ref = tchunk(i, 2, c) if recv else tchunk(i, -1 if up else 1, c)
            to = dev(dx=1 if up else -1)
        else:
            ref = tchunk(i, 0 if not recv else (-1 if k == 0 else 1), c)
            to = dev(dx=1 if k == 0 else -1)
        return rc(ref, ref, tsem.at[0], xr.at[i, k], to)

    def dcopy(i, k, recv):
        ref = tchunk(i, (0, -1, 1, 2)[k], c if not recv else 1 - c)
        return rc(ref, ref, tsem.at[0], dr.at[i, k], partner)

    def ts(i):
        tload(i).wait()
        tcopy(i, 0, False).start()
        tcopy(i, 1, False).start()
        dcopy(i, 0, False).start()

    def tf(i):
        first = i % 2
        tcopy(i, first, True).wait_recv()
        tcopy(i, 2, False).start()
        dcopy(i, 1 + first, False).start()

    def tg(i):
        first = i % 2
        tcopy(i, 1 - first, True).wait_recv()
        dcopy(i, 2 - first, False).start()

    def th(i):
        tcopy(i, 2, True).wait_recv()
        dcopy(i, 3, False).start()

    def td(i):
        for k in range(4):
            dcopy(i, k, True).wait_recv()

    def norm(i, h):
        base = 256 * i + 64 * h

        @pl.loop(0, 2)
        def _(j):
            rows = [pl.ds(pl.multiple_of(base + 32 * j + 16 * g, 16), 16) for g in range(2)]
            averages, scales = [], []
            for r in rows:
                total = T[0, r, :].astype(jnp.float32)
                for k in range(1, 8):
                    total += T[k, r, :].astype(jnp.float32)
                averages.append(jnp.sum(total, axis=1, keepdims=True) * (1.0 / 2048))
            for r, average in zip(rows, averages):
                squares = None
                for k in range(8):
                    centred = T[k, r, :].astype(jnp.float32) - average
                    squares = centred * centred if k == 0 else squares + centred * centred
                variance = jnp.sum(squares, axis=1, keepdims=True) * (1.0 / 2048)
                scales.append(lax.rsqrt(variance + 1e-05))
            for k in range(8):
                cols = slice(256 * k, 256 * k + 256)
                for r, average, scale in zip(rows, averages, scales):
                    centred = T[k, r, :].astype(jnp.float32) - average
                    N[r, cols] = (centred * scale * gain[:, cols]).astype(jnp.bfloat16)

    def part(i, pairs):
        rows = slice(256 * i, 256 * i + 256)
        qkv = ibc = None
        for d, e in pairs:
            one = pl.multiple_of(128 * origin(0, d), 128)
            two = pl.multiple_of(128 * origin(0 if d == 0 else 1, e), 128)
            left = jnp.concatenate([N[rows, pl.ds(one, 128)], N[rows, pl.ds(two, 128)]], axis=1)
            for buf in (B0, B1):
                right = jnp.concatenate([buf[pl.ds(one, 128), :], buf[pl.ds(two, 128), :]], axis=0)
                term = jnp.dot(left, right, preferred_element_type=jnp.float32)
                if buf is B0:
                    qkv = term if qkv is None else qkv + term
                else:
                    ibc = term if ibc is None else ibc + term
        return qkv, ibc

    def pe(i):
        rows = slice(256 * i, 256 * i + 256)
        qkv, ibc = part(i, [(d, d) for d in range(1, EARLY + 1)])
        PACC[rows, 0:256] = qkv
        PACC[rows, 256:640] = ibc

    def proj(i):
        rows = slice(256 * i, 256 * i + 256)
        qkv, ibc = part(i, [(d, d) for d in range(EARLY + 1, 8)] + [(0, 8)])
        qkv = (qkv + PACC[rows, 0:256]).astype(jnp.bfloat16)
        ibc = (ibc + PACC[rows, 256:640]).astype(jnp.bfloat16)
        Q[rows, :] = qkv[:, 0:128]
        KV[128 + 256 * i : 128 + 256 * i + 256, :] = qkv[:, 128:256]
        inner = ibc[:, 0:128].astype(jnp.float32)
        gate_c = ibc[:, 256:384].astype(jnp.float32)
        product = (gate_c * inner).astype(jnp.bfloat16)
        PR[16 + 256 * i : 16 + 256 * i + 256, :] = product.astype(jnp.float32)
        GB[rows, :] = ibc[:, 128:256]

    def halo(k):
        to = dev(dz=1)
        if k == 0:
            return rc(KV.at[1024:1152, :], KV.at[0:128, :], hsem.at[0], hr.at[0], to)
        return rc(PR.at[1032:1040, :], PR.at[8:16, :], hsem.at[1], hr.at[1], to)

    def bias_init():
        row = lax.broadcasted_iota(jnp.int32, (128, 512), 0)
        col = lax.broadcasted_iota(jnp.int32, (128, 512), 1)
        upper = col >= 256
        distance = 128 + row - jnp.where(upper, col - 256, col)
        head = jnp.where(upper, 1, 0) + 2 * t
        slope = jnp.exp2((head + 1).astype(jnp.float32) * (-8.0 / HEADS))
        keep = (distance >= 0) & (distance < WINDOW)
        BIAS[...] = jnp.where(keep, -slope * distance.astype(jnp.float32), -jnp.inf)

    def mix(k):
        for u in (0, 1):
            mix_half(k, u)

    def mix_half(k, u):
        q0 = pl.multiple_of(256 * lax.rem(x + k, NX) + 128 * u, 128)
        lane = lax.broadcasted_iota(jnp.int32, (256, 128), 1)
        low = lane < 64
        q = Q[pl.ds(q0, 128), :]
        kv = KV[pl.ds(q0, 256), :].astype(jnp.float32)
        vk = pltpu.roll(kv, 64, 1)
        keys = jnp.concatenate(
            [jnp.where(low, kv, 0.0), jnp.where(low, 0.0, vk)], axis=0
        ).astype(jnp.bfloat16)
        values = jnp.concatenate(
            [jnp.where(low, vk, 0.0), jnp.where(low, 0.0, kv)], axis=0
        ).astype(jnp.bfloat16)
        scores = lax.dot_general(q, keys, NT, preferred_element_type=jnp.float32)
        scores = scores * HEAD ** (-0.5) + BIAS[...]
        if u == 0:
            col = lax.broadcasted_iota(jnp.int32, (128, 512), 1)
            place = jnp.bitwise_and(col, 255) + (1024 * z + q0 - WINDOW)
            scores = jnp.where(place >= 0, scores, -jnp.inf)
        weights = []
        for g in range(2):
            part = scores[:, 256 * g : 256 * g + 256]
            sink = sinks[0, g]
            top = jnp.maximum(jnp.max(part, axis=1, keepdims=True), sink)
            raised = jnp.exp(part - top)
            below = jnp.sum(raised, axis=1, keepdims=True) + jnp.exp(sink - top)
            weights.append((raised * (1.0 / below)).astype(jnp.bfloat16))
        attended = jnp.dot(
            jnp.concatenate(weights, axis=1), values, preferred_element_type=jnp.float32
        )
        half = slice(128 * u, 128 * u + 128)
        AOUT[k, half, 0:128] = attended.astype(jnp.bfloat16)
        around = PR[pl.ds(pl.multiple_of(q0 + 8, 8), 136), :]
        tap = taps[...].astype(jnp.float32)
        filtered = (
            tap[0:1] * around[6:134] + tap[1:2] * around[7:135] + tap[2:3] * around[8:136]
        )
        gate_b = GB[pl.ds(q0, 128), :].astype(jnp.float32)
        AOUT[k, half, 128:256] = (gate_b * filtered).astype(jnp.bfloat16)

    def acopy(k, u):
        half = pl.ds(128 * u, 128)
        if k == 2:
            return rc(AOUT.at[k, half, :], RLY.at[u], asem.at[0], rr.at[u], dev(dx=1 - 2 * u))
        return rc(AOUT.at[k, half, :], AALL.at[NX - k, half, :], asem.at[0], ar.at[k - 1, u], dev(dx=k))

    def relay(u):
        half = pl.ds(128 * u, 128)
        return rc(RLY.at[u], AALL.at[2, half, :], asem.at[1], ar.at[1, u], dev(dx=1 - 2 * u))

    def out_dot(left, buf, n, at):
        right = buf[512 * n : 512 * n + 512, at : at + 256]
        return lax.dot_general(left, right, NT, preferred_element_type=jnp.float32)

    def excopy(n):
        return rc(XS.at[n], XR.at[n], es.at[0], er.at[n], partner)

    def store(n):
        cols = slice(512 * n, 512 * n + 512)
        return pltpu.make_async_copy(OUTV.at[:, cols], out.at[:, cols], osem.at[n])

    def start():
        bias_init()

    def ox():
        for k in range(3):
            oxcopy(k).start()

    def oxw():
        for k in range(3):
            oxcopy(k).wait_recv()

    def xw(d):
        xl_wait(d - 1)

    def hs():
        halo(0).start()
        halo(1).start()

    def hw():
        halo(0).wait_recv()
        halo(1).wait_recv()
        PR[8:16, :] = jnp.where(z > 0, PR[8:16, :], 0.0)

    def asend(k):
        for u in (0, 1):
            acopy(k, u).start()

    def af(u):
        acopy(2, u).wait_recv()
        relay(u).start()

    def aw(k):
        for u in (0, 1):
            (relay(u) if k == 2 else acopy(k, u)).wait_recv()

    def f0():
        for n in range(4):
            ACC[:, 512 * n : 512 * n + 512] = out_dot(AOUT[0], B3, n, 0)

    def f1():
        for n in range(4):
            ACC[:, 512 * n : 512 * n + 512] += out_dot(AALL[1], B4, n, 0)

    def f3():
        for n in range(4):
            ACC[:, 512 * n : 512 * n + 512] += out_dot(AALL[3], B4, n, 256)

    def ft():
        rows = pl.ds(pl.multiple_of(128 * (1 - c), 128), 128)
        for n in range(4):
            total = ACC[rows, 512 * n : 512 * n + 512] + out_dot(AALL[2, rows, :], B2, n, 0)
            XS[n] = total.astype(jnp.bfloat16)
            if n >= 1:
                excopy(n - 1).start()

    def fo():
        rows = pl.ds(pl.multiple_of(128 * c, 128), 128)
        for n in range(4):
            cols = slice(512 * n, 512 * n + 512)
            ACC[rows, cols] += out_dot(AALL[2, rows, :], B2, n, 0)
            if n == 0:
                excopy(3).start()

    def comb():
        rows = pl.ds(pl.multiple_of(128 * c, 128), 128)
        for n in range(4):
            cols = slice(512 * n, 512 * n + 512)
            excopy(n).wait_recv()
            OUTV[:, cols] = (ACC[rows, cols] + XR[n].astype(jnp.float32)).astype(jnp.bfloat16)
            if n >= 1:
                store(n - 1).start()

    order = (
        (start,), (zs, 0), (ox,), (ts, 1), (ay, 3), (zs, 1), (ys, 0, 0), (ys, 1, 0), (zv, 0, 1), (oxw,), (ts, 0),
        (zs, 2), (ay, 4), (ayf, 3), (zv, 1, 1), (ts, 3), (zv, 0, 2), (ayf, 4), (ts, 2), (zv, 2, 1), (ys, 1, 1),
        (zv, 1, 2), (aye, 3), (zv, 0, 3), (tg, 0), (yf, 1, 0), (aye, 4), (tf, 0), (ys, 1, 2), (ys, 0, 3), (zv, 1, 3),
        (ys, 0, 2), (zv, 2, 2), (tf, 3), (tg, 3), (ys, 1, 3), (zv, 0, 4), (zv, 3, 1), (ys, 0, 1), (yf, 1, 2),
        (zv, 4, 1), (yf, 1, 1), (zv, 1, 4), (zv, 2, 3), (ys, 1, 4), (yf, 0, 3), (zv, 0, 5), (ys, 0, 5), (tf, 2),
        (tf, 1), (th, 3), (ys, 0, 4), (zv, 3, 2), (th, 0), (ys, 2, 0), (yn, 1, 2), (yf, 0, 2), (yf, 0, 0), (ys, 2, 3),
        (zv, 4, 2), (zv, 2, 4), (zv, 1, 5), (yf, 1, 3), (ys, 1, 5), (yf, 0, 4), (td, 3), (yf, 0, 1), (ys, 2, 4),
        (tg, 2), (yf, 0, 5), (norm, 3, 2), (yf, 1, 4), (th, 2), (yn, 0, 3), (zv, 3, 3), (zv, 0, 6), (zv, 0, 7),
        (ys, 0, 6), (norm, 3, 3), (norm, 3, 0), (yn, 0, 0), (th, 1), (tg, 1), (zv, 2, 5), (yn, 1, 1), (ys, 0, 7),
        (td, 2), (norm, 2, 0), (norm, 2, 3), (zv, 1, 6), (zv, 4, 3), (td, 0), (ys, 1, 6), (td, 1), (norm, 1, 1),
        (yf, 1, 5), (yn, 0, 5), (zv, 1, 7), (yn, 0, 1), (yn, 1, 3), (ys, 1, 7), (zv, 3, 4), (yn, 0, 2), (yn, 1, 4),
        (norm, 1, 0), (norm, 0, 1), (yn, 0, 4), (norm, 0, 3), (xw, 1), (zv, 0, 8), (norm, 3, 1), (norm, 0, 0),
        (yf, 0, 6), (zv, 2, 6), (ys, 0, 8), (xw, 3), (norm, 0, 2), (yf, 1, 6), (norm, 1, 3), (zv, 2, 7), (zv, 4, 4),
        (yn, 1, 0), (zv, 1, 8), (yn, 0, 7), (ys, 1, 8), (zv, 3, 5), (norm, 1, 2), (pe, 1), (norm, 2, 1), (yn, 1, 5),
        (pe, 3), (xw, 4), (yf, 2, 4), (ys, 2, 1), (norm, 2, 2), (ys, 2, 6), (pe, 0), (yn, 1, 6), (yn, 1, 7),
        (yn, 0, 8), (yf, 2, 3), (yn, 0, 6), (yn, 1, 8), (proj, 3), (ys, 2, 5), (hs,), (zv, 3, 6), (pe, 2), (ys, 2, 2),
        (ys, 2, 7), (proj, 0), (proj, 2), (proj, 1), (yn, 2, 3), (xw, 5), (zv, 4, 5), (zv, 3, 7), (zv, 2, 8), (hw,),
        (mix, 2), (asend, 2), (yf, 2, 5), (mix, 3), (asend, 3), (mix, 1), (asend, 1), (yf, 2, 0), (yf, 2, 6),
        (yf, 2, 1), (yn, 2, 4), (mix, 0), (ys, 2, 8), (zv, 3, 8), (zv, 4, 6), (xw, 7), (yn, 2, 5), (f0,), (yf, 2, 2),
        (xw, 2), (af, 0), (xw, 6), (af, 1), (aw, 3), (yn, 2, 2), (yn, 2, 1), (yn, 2, 6), (aw, 1), (yn, 2, 7),
        (zv, 4, 8), (zv, 4, 7), (yn, 2, 8), (yn, 2, 0), (xw, 8), (f1,), (f3,), (aw, 2), (ft,), (fo,), (comb,),
    )
    for event, *where in order:
        with jax.named_scope(event.__name__ + "_".join(map(str, where))):
            event(*where)
    with jax.named_scope("tail"):
        store(3).start()

    def sent(ref, sem):
        pltpu.make_async_copy(ref, ref, sem).wait()

    with jax.named_scope("sent"):
        for st in (0, 1, 2):
            sent(bufs[st].at[0:2016, :], ss.at[st])
        sent(B3.at[0:2016, :], ss.at[3])
        sent(B4.at[0 : 96 + 15 * (128 - LATE), :], ss.at[4])
        sent(B3.at[0 : 96 + 15 * LATE, :], ss.at[5])
        sent(B3.at[0 : 15 * LATE, :], ss.at[6])
        sent(T.at[0:7], tsem.at[0])
        for k in range(2):
            halo(k).wait_send()
        sent(AOUT.at[0:3], asem.at[0])
        sent(RLY, asem.at[1])
        sent(XS, es.at[0])
    with jax.named_scope("stored"):
        for n in range(4):
            store(n).wait()


def on_device(
    tokens, norm_gain, w_query, w_key, w_value, w_conv_in, w_conv_b, w_conv_c,
    conv_taps, sink_logits, w_attn_out, w_conv_out,
):
    vmem = pl.BlockSpec(memory_space=pltpu.VMEM)
    smem = pl.BlockSpec(memory_space=pltpu.SMEM)
    hbm = pl.BlockSpec(memory_space=pl.ANY)
    bf, f32 = jnp.bfloat16, jnp.float32
    dma = pltpu.SemaphoreType.DMA
    V = pltpu.VMEM
    result = pl.pallas_call(
        kernel,
        out_shape=jax.ShapeDtypeStruct((128, 2048), bf),
        in_specs=[hbm] + [vmem] * 8 + [smem] + [vmem] * 2,
        out_specs=hbm,
        scratch_shapes=[
            V((8, 1024, 256), bf), V((1024, 2048), bf),
            V((2048, 256), bf), V((2048, 384), bf), V((2048, 256), bf), V((2048, 256), bf), V((2048, 512), bf),
            V((1024, 128), bf), V((1152, 128), bf), V((1040, 128), f32), V((1024, 128), bf),
            V((128, 512), f32), V((4, 256, 256), bf), V((4, 256, 256), bf), V((2, 128, 256), bf),
            V((4, 128, 512), bf), V((4, 128, 512), bf), V((256, 2048), f32), V((128, 2048), bf), V((1024, 640), f32),
            dma((4,)), dma((4,)),
            dma((7,)), dma((5, 2, 8)), dma((3, 17, 3)), dma((2, 3)),
            dma((1,)), dma((4, 3)), dma((4, 4)), dma((3,)), dma((2, 2, 8)),
            dma((2,)), dma((2,)), dma((2,)), dma((3, 2)), dma((2,)), dma((1,)), dma((4,)),
        ],
        compiler_params=pltpu.CompilerParams(
            collective_id=0, has_side_effects=True, vmem_limit_bytes=60 * 1024 * 1024
        ),
    )(
        tokens[0], norm_gain[None], w_query, w_key, w_value, w_conv_in, w_conv_b, w_conv_c,
        conv_taps, sink_logits[None], w_attn_out.T, w_conv_out.T,
    )
    return result[None]


def solution(mesh):
    placed = (
        P("fs", "sp", "tp"),
        P(),
        P(("sp", "fs"), "tp"),
        P(("sp", "fs"), "tp"),
        P(("sp", "fs"), "tp"),
        P(("sp", "fs"), "tp"),
        P(("sp", "fs"), "tp"),
        P(("sp", "fs"), "tp"),
        P(None, "tp"),
        P("tp"),
        P("tp", ("sp", "fs")),
        P("tp", ("sp", "fs")),
    )
    return jax.shard_map(
        on_device,
        mesh=mesh,
        in_specs=placed,
        out_specs=P("fs", ("sp", "tp"), None),
        check_vma=False,
    )
```

```python
import functools

import jax
import jax.numpy as jnp
from jax import lax
from jax.experimental import pallas as pl
from jax.experimental.pallas import tpu as pltpu
from jax.sharding import PartitionSpec as P

HEADS = 16
HEAD = 64
WINDOW = 128
NZ, NY, NX = 16, 4, 4
MESH = pl.DeviceIdType.MESH
NT = (((1,), (1,)), ((), ()))

STREAMS = (("zy", 256), ("zy", 384), ("zy", 256), ("yz", 256), ("yz", 512))
UP = (8, 7, 8, 7, 8)
SKIP = ((5, 3), (5, 3), (6, 2), (6, 2), (6, 2))
DIRECT = 8
LATE = 96
EARLY = (1, 2, 3, 4, 5)


def kernel(
    tok, gain_in, wq, wk, wv, wi, wb, wc, taps_in, sinks_in, wao, wco,
    out,
    T, N, B0, B1, B2, B3, B4, Q, KV, PR, GB, BIAS, AALL, AOUT, RLY, XS, XR, ACC, OUTV, PACC, gain, taps, sinks, kvw,
    lsem, wsem, osem, ss, zr, yfr, ynr, ayr, tsem, xr, dr, oxr, xlr, hsem, hr, asem, ar, rr, es, er,
):
    z = lax.axis_index("sp")
    y = lax.axis_index("fs")
    t = lax.axis_index("tp")
    x = t // 2
    c = t % 2
    bufs = (B0, B1, B2, B3, B4)

    def dev(dz=0, dy=0, dx=0):
        return (
            lax.rem(z + NZ + dz, NZ),
            lax.rem(y + NY + dy, NY),
            lax.rem(x + NX + dx, NX) * 2 + c,
        )

    partner = (z, y, x * 2 + (1 - c))

    def rc(src, dst, ssem, rsem, to):
        return pltpu.make_async_remote_copy(
            src_ref=src, dst_ref=dst, send_sem=ssem, recv_sem=rsem, device_id=to, device_id_type=MESH
        )

    barrier = pltpu.get_barrier_semaphore()
    peers = [dev(dz=1), dev(dz=-1), dev(dy=1), dev(dy=-1), dev(dx=1), dev(dx=-1), dev(dx=2), partner]
    for peer in peers:
        pl.semaphore_signal(barrier, inc=1, device_id=peer, device_id_type=MESH)

    own = pl.ds(pl.multiple_of(32 * (NY * z + y), 32), 32)
    whole = (
        (wq, B0, 0), (wi, B1, 0), (wb, B1, 128), (wc, B1, 256), (wao, B3, 0), (wco, B3, 128),
    )
    for src, buf, at in whole:
        pltpu.make_async_copy(src, buf.at[own, at : at + 128], wsem.at[0]).start()
    narrow = [pltpu.make_async_copy(src, kvw.at[k], wsem.at[1 + k]) for k, src in enumerate((wk, wv))]
    small = [
        pltpu.make_async_copy(src, dst, wsem.at[3 + k])
        for k, (src, dst) in enumerate(((gain_in, gain), (taps_in, taps), (sinks_in, sinks)))
    ]

    def tload(i):
        rows = pl.ds(256 * i, 256)
        return pltpu.make_async_copy(tok.at[rows, :], T.at[t, rows, :], lsem.at[i])

    for copy in narrow:
        copy.start()
    for i in range(4):
        tload(i).start()
    for copy in small:
        copy.start()
    for copy in narrow:
        copy.wait()
    B0[own, 128:256] = jnp.concatenate([kvw[0], kvw[1]], axis=1)

    def landed(ref, sem):
        pltpu.make_async_copy(ref, ref, sem).wait()

    landed(B1.at[0:64, :], wsem.at[0])
    for copy in small:
        copy.wait()
    with jax.named_scope("barrier"):
        pl.semaphore_wait(barrier, len(peers))

    def zblock(st, b):
        buf = bufs[st]
        if STREAMS[st][0] == "zy":
            return buf.at[pl.ds(pl.multiple_of(32 * (NY * b + y), 32), 32), :]
        if st == 4:
            return buf.at[pl.ds(pl.multiple_of(128 * b + LATE, 16), 128 - LATE), :]
        return buf.at[pl.ds(pl.multiple_of(128 * b, 128), 128), :]

    def yblock(st, b, dy):
        yy = lax.rem(y + NY + dy, NY)
        return bufs[st].at[pl.ds(pl.multiple_of(32 * (NY * b + yy), 32), 32), :]

    def steps(st, way):
        return UP[st] if way == 0 else 15 - UP[st]

    def origin(way, s):
        return lax.rem(z + NZ - s, NZ) if way == 0 else lax.rem(z + s, NZ)

    def zpass(st, d):
        near, jump = SKIP[st]
        for way in (0, 1):
            last = steps(st, way)
            ref = zblock(st, origin(way, d))
            for hops in (1, jump):
                to = d + hops
                if hops == 1 and to > min(near, last) or hops > 1 and (d == 0 or not near < to <= last):
                    continue
                if d <= last:
                    rc(
                        ref, ref, ss.at[st], zr.at[st, to - 1], dev(dz=hops if way == 0 else -hops)
                    ).start()

    def zs(st):
        zpass(st, 0)

    def zv(st, d):
        rows = 32 if STREAMS[st][0] == "zy" else 128 - LATE if st == 4 else 128
        ways = sum(d <= steps(st, way) for way in (0, 1))
        landed(bufs[st].at[0 : ways * rows, :], zr.at[st, d - 1])
        zpass(st, d)

    def slots(st, s):
        if s < 0:
            return [(0, 0, 0)]
        return [(1 + 8 * way + s, way, s + 1) for way in (0, 1) if s < steps(st, way)]

    def group(st, e):
        return 0 if st == 2 or e in EARLY else 1

    def y_start(st, slot, b, d, k):
        up = slot < 9
        if k == 2:
            ref = yblock(st, b, 0 if d >= DIRECT else -1 if up else 1)
            to = dev(dy=2 if d >= DIRECT else 1 if up else -1)
        else:
            ref = yblock(st, b, 0)
            to = dev(dy=1 - 2 * k)
        forwards = d < DIRECT and k == (0 if up else 1)
        sem = yfr.at[st, d] if forwards else ynr.at[st, group(st, d)]
        rc(ref, ref, ss.at[st], sem, to).start()

    def ys(st, e):
        for slot, way, d in slots(st, e - 1):
            for k in (0, 1, 2) if e >= DIRECT else (0, 1):
                y_start(st, slot, origin(way, d), d, k)

    def yf(st, e):
        blocks = slots(st, e - 1)
        landed(bufs[st].at[0 : 32 * len(blocks), :], yfr.at[st, e])
        for slot, way, d in blocks:
            y_start(st, slot, origin(way, d), d, 2)

    def yw(st, g):
        count = sum(
            len(slots(st, e - 1)) * (3 if e >= DIRECT else 2) for e in range(9) if group(st, e) == g
        )
        landed(bufs[st].at[0 : 32 * count, :], ynr.at[st, g])

    def ay_start(st, k):
        up = st % 2 == 0
        if k == 2:
            ref = yblock(st, z, -1 if up else 1)
            to = dev(dy=1 if up else -1)
        else:
            ref = yblock(st, z, 0)
            to = dev(dy=1 - 2 * k)
        rc(ref, ref, ss.at[st], ayr.at[st - 3, 0 if k == (0 if up else 1) else 1], to).start()

    def ay(st):
        ay_start(st, 0)
        ay_start(st, 1)

    def ayf(st):
        landed(bufs[st].at[0:32, :], ayr.at[st - 3, 0])
        ay_start(st, 2)

    def aye(st):
        landed(bufs[st].at[0:64, :], ayr.at[st - 3, 1])
        zs(st)

    ox_parts = ((1, 4, 0), (2, 2, 0), (3, 4, 256))

    def oxcopy(k):
        d, st, at = ox_parts[k]
        return rc(B3.at[own, :], bufs[st].at[own, at : at + 256], ss.at[5], oxr.at[0], dev(dx=-d))

    def xlcopy(s, way, k):
        rows = pl.ds(pl.multiple_of(128 * origin(way, s + 1), 128), LATE)
        at = 256 * k
        return rc(
            B3.at[rows, :], B4.at[rows, at : at + 256], ss.at[5 + k], xlr.at[0], dev(dx=-1 if k == 0 else 1)
        )

    def xl_send(s):
        for way in (0, 1):
            if s < steps(3, way):
                for k in (0, 1):
                    xlcopy(s, way, k).start()

    def tchunk(i, dx, cc):
        tt = lax.rem(x + NX + dx, NX) * 2 + cc
        return T.at[tt, pl.ds(256 * i, 256), :]

    def tcopy(i, k, recv):
        up = i % 2 == 0
        if k == 2:
            ref = tchunk(i, 2, c) if recv else tchunk(i, -1 if up else 1, c)
            to = dev(dx=1 if up else -1)
        else:
            ref = tchunk(i, 0 if not recv else (-1 if k == 0 else 1), c)
            to = dev(dx=1 if k == 0 else -1)
        return rc(ref, ref, tsem.at[0], xr.at[i, k], to)

    def dcopy(i, k, recv):
        ref = tchunk(i, (0, -1, 1, 2)[k], c if not recv else 1 - c)
        return rc(ref, ref, tsem.at[0], dr.at[i], partner)

    def ts(i):
        tload(i).wait()
        tcopy(i, 0, False).start()
        tcopy(i, 1, False).start()
        dcopy(i, 0, False).start()

    def tf(i):
        first = i % 2
        tcopy(i, first, True).wait_recv()
        tcopy(i, 2, False).start()
        dcopy(i, 1 + first, False).start()

    def tg(i):
        first = i % 2
        tcopy(i, 1 - first, True).wait_recv()
        dcopy(i, 2 - first, False).start()

    def th(i):
        tcopy(i, 2, True).wait_recv()
        dcopy(i, 3, False).start()

    def td(i):
        landed(T.at[0], dr.at[i])

    def norm(i, h):
        rows = slice(256 * i + 128 * h, 256 * i + 128 * h + 128)
        total = T[0, rows, :].astype(jnp.float32)
        for k in range(1, 8):
            total += T[k, rows, :].astype(jnp.float32)
        average = jnp.sum(total, axis=1, keepdims=True) * (1.0 / 2048)
        squares = None
        for k in range(8):
            centred = T[k, rows, :].astype(jnp.float32) - average
            squares = centred * centred if k == 0 else squares + centred * centred
        variance = jnp.sum(squares, axis=1, keepdims=True) * (1.0 / 2048)
        scale = lax.rsqrt(variance + 1e-05)
        for k in range(8):
            cols = slice(256 * k, 256 * k + 256)
            centred = T[k, rows, :].astype(jnp.float32) - average
            N[rows, cols] = (centred * scale * gain[:, cols]).astype(jnp.bfloat16)

    def part(i, pairs):
        rows = slice(256 * i, 256 * i + 256)
        qkv = ibc = None
        for d, e in pairs:
            one = pl.multiple_of(128 * origin(0, d), 128)
            two = pl.multiple_of(128 * origin(0 if d == 0 else 1, e), 128)
            left = jnp.concatenate([N[rows, pl.ds(one, 128)], N[rows, pl.ds(two, 128)]], axis=1)
            for buf in (B0, B1):
                right = jnp.concatenate([buf[pl.ds(one, 128), :], buf[pl.ds(two, 128), :]], axis=0)
                term = jnp.dot(left, right, preferred_element_type=jnp.float32)
                if buf is B0:
                    qkv = term if qkv is None else qkv + term
                else:
                    ibc = term if ibc is None else ibc + term
        return qkv, ibc

    def pe(i):
        rows = slice(256 * i, 256 * i + 256)
        qkv, ibc = part(i, [(d, d) for d in EARLY])
        PACC[rows, 0:256] = qkv
        PACC[rows, 256:640] = ibc

    def proj(i):
        rows = slice(256 * i, 256 * i + 256)
        qkv, ibc = part(i, [(d, d) for d in range(1, 8) if d not in EARLY] + [(0, 8)])
        qkv = (qkv + PACC[rows, 0:256]).astype(jnp.bfloat16)
        ibc = (ibc + PACC[rows, 256:640]).astype(jnp.bfloat16)
        Q[rows, :] = qkv[:, 0:128]
        KV[128 + 256 * i : 128 + 256 * i + 256, :] = qkv[:, 128:256]
        inner = ibc[:, 0:128].astype(jnp.float32)
        gate_c = ibc[:, 256:384].astype(jnp.float32)
        product = (gate_c * inner).astype(jnp.bfloat16)
        PR[16 + 256 * i : 16 + 256 * i + 256, :] = product.astype(jnp.float32)
        GB[rows, :] = ibc[:, 128:256]

    def halo(k):
        to = dev(dz=1)
        if k == 0:
            return rc(KV.at[1024:1152, :], KV.at[0:128, :], hsem.at[0], hr.at[0], to)
        return rc(PR.at[1032:1040, :], PR.at[8:16, :], hsem.at[1], hr.at[1], to)

    def bias_init():
        row = lax.broadcasted_iota(jnp.int32, (128, 512), 0)
        col = lax.broadcasted_iota(jnp.int32, (128, 512), 1)
        upper = col >= 256
        distance = 128 + row - jnp.where(upper, col - 256, col)
        head = jnp.where(upper, 1, 0) + 2 * t
        slope = jnp.exp2((head + 1).astype(jnp.float32) * (-8.0 / HEADS))
        keep = (distance >= 0) & (distance < WINDOW)
        BIAS[...] = jnp.where(keep, -slope * distance.astype(jnp.float32), -jnp.inf)

    def mix(k):
        for u in (0, 1):
            mix_half(k, u)

    def mix_half(k, u):
        q0 = pl.multiple_of(256 * lax.rem(x + k, NX) + 128 * u, 128)
        lane = lax.broadcasted_iota(jnp.int32, (256, 128), 1)
        low = lane < 64
        q = Q[pl.ds(q0, 128), :]
        kv = KV[pl.ds(q0, 256), :].astype(jnp.float32)
        vk = pltpu.roll(kv, 64, 1)
        keys = jnp.concatenate(
            [jnp.where(low, kv, 0.0), jnp.where(low, 0.0, vk)], axis=0
        ).astype(jnp.bfloat16)
        values = jnp.concatenate(
            [jnp.where(low, vk, 0.0), jnp.where(low, 0.0, kv)], axis=0
        ).astype(jnp.bfloat16)
        scores = lax.dot_general(q, keys, NT, preferred_element_type=jnp.float32)
        scores = scores * HEAD ** (-0.5) + BIAS[...]
        if u == 0:
            col = lax.broadcasted_iota(jnp.int32, (128, 512), 1)
            place = jnp.bitwise_and(col, 255) + (1024 * z + q0 - WINDOW)
            scores = jnp.where(place >= 0, scores, -jnp.inf)
        weights = []
        for g in range(2):
            part = scores[:, 256 * g : 256 * g + 256]
            sink = sinks[0, g]
            top = jnp.maximum(jnp.max(part, axis=1, keepdims=True), sink)
            raised = jnp.exp(part - top)
            below = jnp.sum(raised, axis=1, keepdims=True) + jnp.exp(sink - top)
            weights.append((raised * (1.0 / below)).astype(jnp.bfloat16))
        attended = jnp.dot(
            jnp.concatenate(weights, axis=1), values, preferred_element_type=jnp.float32
        )
        half = slice(128 * u, 128 * u + 128)
        AOUT[k, half, 0:128] = attended.astype(jnp.bfloat16)
        around = PR[pl.ds(pl.multiple_of(q0 + 8, 8), 136), :]
        tap = taps[...].astype(jnp.float32)
        filtered = (
            tap[0:1] * around[6:134] + tap[1:2] * around[7:135] + tap[2:3] * around[8:136]
        )
        gate_b = GB[pl.ds(q0, 128), :].astype(jnp.float32)
        AOUT[k, half, 128:256] = (gate_b * filtered).astype(jnp.bfloat16)

    def acopy(k, u):
        half = pl.ds(128 * u, 128)
        if k == 2:
            return rc(AOUT.at[k, half, :], RLY.at[u], asem.at[0], rr.at[u], dev(dx=1 - 2 * u))
        return rc(AOUT.at[k, half, :], AALL.at[NX - k, half, :], asem.at[0], ar.at[k - 1], dev(dx=k))

    def relay(u):
        half = pl.ds(128 * u, 128)
        return rc(RLY.at[u], AALL.at[2, half, :], asem.at[1], ar.at[1], dev(dx=1 - 2 * u))

    def out_dot(left, buf, n, at):
        right = buf[512 * n : 512 * n + 512, at : at + 256]
        return lax.dot_general(left, right, NT, preferred_element_type=jnp.float32)

    def excopy(n):
        return rc(XS.at[n], XR.at[n], es.at[0], er.at[n], partner)

    def store(n):
        cols = slice(512 * n, 512 * n + 512)
        return pltpu.make_async_copy(OUTV.at[:, cols], out.at[:, cols], osem.at[0])

    def start():
        bias_init()

    def ox():
        for k in range(3):
            oxcopy(k).start()

    def oxw():
        landed(B3.at[0:96, :], oxr.at[0])

    def xs(d):
        xl_send(d - 1)

    def xw():
        landed(B4.at[0 : 15 * LATE, :], xlr.at[0])

    def hs():
        halo(0).start()
        halo(1).start()

    def hw():
        halo(0).wait_recv()
        halo(1).wait_recv()
        PR[8:16, :] = jnp.where(z > 0, PR[8:16, :], 0.0)

    def asend(k):
        for u in (0, 1):
            acopy(k, u).start()

    def af(u):
        acopy(2, u).wait_recv()
        relay(u).start()

    def aw(k):
        landed(AALL.at[0], ar.at[k - 1])

    def f0():
        for n in range(4):
            ACC[:, 512 * n : 512 * n + 512] = out_dot(AOUT[0], B3, n, 0)

    def f1():
        for n in range(4):
            ACC[:, 512 * n : 512 * n + 512] += out_dot(AALL[1], B4, n, 0)

    def f3():
        for n in range(4):
            ACC[:, 512 * n : 512 * n + 512] += out_dot(AALL[3], B4, n, 256)

    def ft():
        rows = pl.ds(pl.multiple_of(128 * (1 - c), 128), 128)
        for n in range(4):
            total = ACC[rows, 512 * n : 512 * n + 512] + out_dot(AALL[2, rows, :], B2, n, 0)
            XS[n] = total.astype(jnp.bfloat16)
            if n >= 1:
                excopy(n - 1).start()

    def fo():
        rows = pl.ds(pl.multiple_of(128 * c, 128), 128)
        for n in range(4):
            cols = slice(512 * n, 512 * n + 512)
            ACC[rows, cols] += out_dot(AALL[2, rows, :], B2, n, 0)
            if n == 0:
                excopy(3).start()

    def comb():
        rows = pl.ds(pl.multiple_of(128 * c, 128), 128)
        for n in range(4):
            cols = slice(512 * n, 512 * n + 512)
            excopy(n).wait_recv()
            OUTV[:, cols] = (ACC[rows, cols] + XR[n].astype(jnp.float32)).astype(jnp.bfloat16)
            if n >= 1:
                store(n - 1).start()

    order = (
        (start,), (ay, 3), (zs, 0), (zs, 1), (ys, 1, 0), (ys, 0, 0), (ox,), (ts, 2), (ayf, 3), (oxw,), (zs, 2),
        (ts, 0), (ay, 4), (ts, 3), (zv, 0, 1), (zv, 1, 1), (yf, 0, 0), (ys, 0, 1), (aye, 3), (yf, 1, 0), (ayf, 4),
        (zv, 2, 1), (tf, 2), (ys, 1, 1), (zv, 0, 2), (zv, 1, 2), (ys, 0, 2), (zv, 3, 1), (tg, 0), (ts, 1), (aye, 4),
        (zv, 2, 2), (zv, 0, 3), (ys, 1, 2), (zv, 1, 3), (ys, 0, 3), (tf, 0), (ys, 2, 0), (yf, 0, 1), (zv, 3, 2),
        (tf, 3), (zv, 4, 1), (yf, 1, 1), (tf, 1), (ys, 1, 3), (zv, 0, 4), (ys, 0, 4), (zv, 1, 4), (zv, 2, 3),
        (ys, 1, 4), (tg, 2), (th, 2), (yf, 1, 2), (td, 2), (zv, 1, 6), (ys, 1, 6), (norm, 2, 0), (zv, 3, 3), (xs, 2),
        (zv, 0, 6), (yf, 0, 4), (zv, 4, 2), (th, 0), (yf, 1, 3), (zv, 0, 5), (ys, 0, 5), (yf, 1, 4), (th, 3),
        (yf, 0, 2), (zv, 1, 5), (zv, 0, 7), (th, 1), (tg, 1), (ys, 0, 7), (ys, 1, 5), (zv, 2, 4), (yf, 1, 6), (xs, 1),
        (td, 1), (ys, 0, 6), (zv, 1, 7), (zv, 3, 4), (norm, 1, 1), (yf, 0, 3), (ys, 1, 7), (norm, 2, 1), (yf, 1, 5),
        (xs, 3), (zv, 4, 3), (tg, 3), (yf, 0, 5), (td, 0), (zv, 1, 8), (zv, 0, 8), (ys, 0, 8), (yf, 0, 6), (td, 3),
        (zv, 2, 5), (norm, 0, 1), (xs, 4), (ys, 1, 8), (zv, 3, 5), (yf, 0, 7), (yf, 2, 0), (norm, 0, 0), (yw, 1, 0),
        (yw, 0, 0), (yf, 1, 7), (pe, 0), (ys, 2, 2), (norm, 1, 0), (pe, 2), (norm, 3, 0), (ys, 2, 4), (pe, 1),
        (norm, 3, 1), (xs, 5), (zv, 4, 4), (ys, 2, 1), (yw, 0, 1), (pe, 3), (yw, 1, 1), (zv, 2, 7), (proj, 3),
        (ys, 2, 3), (hs,), (zv, 2, 6), (yf, 2, 2), (zv, 3, 6), (proj, 2), (ys, 2, 5), (xs, 6), (proj, 1), (ys, 2, 6),
        (ys, 2, 7), (proj, 0), (zv, 3, 7), (xs, 7), (yf, 2, 4), (zv, 4, 5), (yf, 2, 1), (hw,), (mix, 2), (asend, 2),
        (zv, 2, 8), (mix, 1), (zv, 3, 8), (ys, 2, 8), (yf, 2, 5), (yf, 2, 7), (xs, 8), (asend, 1), (yf, 2, 3),
        (mix, 3), (asend, 3), (zv, 4, 6), (mix, 0), (af, 0), (yf, 2, 6), (af, 1), (f0,), (aw, 3), (zv, 4, 7), (xw,),
        (yw, 2, 0), (aw, 1), (zv, 4, 8), (f1,), (f3,), (aw, 2), (ft,), (fo,), (comb,),
    )
    for event, *where in order:
        with jax.named_scope(event.__name__ + "_".join(map(str, where))):
            event(*where)
    with jax.named_scope("tail"):
        store(3).start()

    def sent(ref, sem):
        pltpu.make_async_copy(ref, ref, sem).wait()

    with jax.named_scope("sent"):
        for st in (0, 1, 2):
            sent(bufs[st].at[0:2016, :], ss.at[st])
        sent(B3.at[0:2016, :], ss.at[3])
        sent(B4.at[0 : 96 + 15 * (128 - LATE), :], ss.at[4])
        sent(B3.at[0 : 96 + 15 * LATE, :], ss.at[5])
        sent(B3.at[0 : 15 * LATE, :], ss.at[6])
        sent(T.at[0:7], tsem.at[0])
        for k in range(2):
            halo(k).wait_send()
        sent(AOUT.at[0:3], asem.at[0])
        sent(RLY, asem.at[1])
        sent(XS, es.at[0])
    with jax.named_scope("stored"):
        pltpu.make_async_copy(OUTV, out, osem.at[0]).wait()


def on_device(
    tokens, norm_gain, w_query, w_key, w_value, w_conv_in, w_conv_b, w_conv_c,
    conv_taps, sink_logits, w_attn_out, w_conv_out,
):
    hbm = pl.BlockSpec(memory_space=pl.ANY)
    bf, f32 = jnp.bfloat16, jnp.float32
    dma = pltpu.SemaphoreType.DMA
    V = pltpu.VMEM
    result = pl.pallas_call(
        kernel,
        out_shape=jax.ShapeDtypeStruct((128, 2048), bf),
        in_specs=[hbm] * 12,
        out_specs=hbm,
        scratch_shapes=[
            V((8, 1024, 256), bf), V((1024, 2048), bf),
            V((2048, 256), bf), V((2048, 384), bf), V((2048, 256), bf), V((2048, 256), bf), V((2048, 512), bf),
            V((1024, 128), bf), V((1152, 128), bf), V((1040, 128), f32), V((1024, 128), bf),
            V((128, 512), f32), V((4, 256, 256), bf), V((4, 256, 256), bf), V((2, 128, 256), bf),
            V((4, 128, 512), bf), V((4, 128, 512), bf), V((256, 2048), f32), V((128, 2048), bf), V((1024, 640), f32),
            V((1, 2048), f32), V((3, 128), bf), pltpu.SMEM((1, 2), f32), V((2, 32, 64), bf),
            dma((4,)), dma((6,)), dma((1,)),
            dma((7,)), dma((5, 8)), dma((3, max(DIRECT, 1))), dma((3, 2)), dma((2, 2)),
            dma((1,)), dma((4, 3)), dma((4,)), dma((1,)), dma((1,)),
            dma((2,)), dma((2,)), dma((2,)), dma((3,)), dma((2,)), dma((1,)), dma((4,)),
        ],
        compiler_params=pltpu.CompilerParams(
            collective_id=0, has_side_effects=True, vmem_limit_bytes=60 * 1024 * 1024
        ),
    )(
        tokens[0], norm_gain[None], w_query, w_key, w_value, w_conv_in, w_conv_b, w_conv_c,
        conv_taps, sink_logits[None], w_attn_out.T, w_conv_out.T,
    )
    return result[None]


def solution(mesh):
    placed = (
        P("fs", "sp", "tp"),
        P(),
        P(("sp", "fs"), "tp"),
        P(("sp", "fs"), "tp"),
        P(("sp", "fs"), "tp"),
        P(("sp", "fs"), "tp"),
        P(("sp", "fs"), "tp"),
        P(("sp", "fs"), "tp"),
        P(None, "tp"),
        P("tp"),
        P("tp", ("sp", "fs")),
        P("tp", ("sp", "fs")),
    )
    return jax.shard_map(
        on_device,
        mesh=mesh,
        in_specs=placed,
        out_specs=P("fs", ("sp", "tp"), None),
        check_vma=False,
    )
```

```python
import functools

import jax
import jax.numpy as jnp
from jax import lax
from jax.experimental import pallas as pl
from jax.experimental.pallas import tpu as pltpu
from jax.sharding import PartitionSpec as P

HEADS = 16
HEAD = 64
WINDOW = 128
NZ, NY, NX = 16, 4, 4
MESH = pl.DeviceIdType.MESH
NT = (((1,), (1,)), ((), ()))

STREAMS = (("zy", 256), ("zy", 384), ("zy", 256), ("yz", 256), ("yz", 512), ("yz", 256))
UP = (8, 7, 8, 7, 8, 7)
SKIP = ((6, 2), (6, 2), (6, 2), (6, 2), (6, 2), (6, 2))
DIRECT = 7
LATE = 80
EARLY = (1, 2, 3, 4, 5)


def kernel(
    tok, gain_in, wq, wk, wv, wi, wb, wc, taps_in, sinks_in, wao, wco,
    out,
    T, N, B0, B1, B2, B3, B4, Q, KV, PR, GB, BIAS, AALL, AOUT, RLY, XS, XR, ACC, OUTV, PACC, gain, taps, sinks, kvw,
    lsem, wsem, osem, ss, zr, yfr, ynr, ayr, tsem, xr, dr, oxr, xlr, hsem, hr, asem, ar, rr, es, er,
):
    z = lax.axis_index("sp")
    y = lax.axis_index("fs")
    t = lax.axis_index("tp")
    x = t // 2
    c = t % 2
    bufs = (B0, B1, B2, B3, B4, B3)

    def dev(dz=0, dy=0, dx=0):
        return (
            lax.rem(z + NZ + dz, NZ),
            lax.rem(y + NY + dy, NY),
            lax.rem(x + NX + dx, NX) * 2 + c,
        )

    partner = (z, y, x * 2 + (1 - c))

    def rc(src, dst, ssem, rsem, to):
        return pltpu.make_async_remote_copy(
            src_ref=src, dst_ref=dst, send_sem=ssem, recv_sem=rsem, device_id=to, device_id_type=MESH
        )

    barrier = pltpu.get_barrier_semaphore()
    peers = [dev(dz=1), dev(dz=-1), dev(dy=1), dev(dy=-1), dev(dx=1), dev(dx=-1), dev(dx=2), partner]
    for peer in peers:
        pl.semaphore_signal(barrier, inc=1, device_id=peer, device_id_type=MESH)

    own = pl.ds(pl.multiple_of(32 * (NY * z + y), 32), 32)
    whole = (
        (wq, B0, 0), (wi, B1, 0), (wb, B1, 128), (wc, B1, 256), (wao, B3, 0), (wco, B3, 128),
    )
    for src, buf, at in whole:
        pltpu.make_async_copy(src, buf.at[own, at : at + 128], wsem.at[0]).start()
    narrow = [pltpu.make_async_copy(src, kvw.at[k], wsem.at[1 + k]) for k, src in enumerate((wk, wv))]
    small = [
        pltpu.make_async_copy(src, dst, wsem.at[3 + k])
        for k, (src, dst) in enumerate(((gain_in, gain), (taps_in, taps), (sinks_in, sinks)))
    ]

    def tload(i):
        rows = pl.ds(256 * i, 256)
        return pltpu.make_async_copy(tok.at[rows, :], T.at[t, rows, :], lsem.at[i])

    for copy in narrow:
        copy.start()
    for i in range(4):
        tload(i).start()
    for copy in small:
        copy.start()
    for copy in narrow:
        copy.wait()
    B0[own, 128:256] = jnp.concatenate([kvw[0], kvw[1]], axis=1)

    def landed(ref, sem):
        pltpu.make_async_copy(ref, ref, sem).wait()

    landed(B1.at[0:64, :], wsem.at[0])
    for copy in small:
        copy.wait()
    with jax.named_scope("barrier"):
        pl.semaphore_wait(barrier, len(peers))

    def zblock(st, b):
        buf = bufs[st]
        if STREAMS[st][0] == "zy":
            return buf.at[pl.ds(pl.multiple_of(32 * (NY * b + y), 32), 32), :]
        if st == 4:
            return buf.at[pl.ds(pl.multiple_of(128 * b + LATE, 16), 128 - LATE), :]
        return buf.at[pl.ds(pl.multiple_of(128 * b + (64 if st == 5 else 0), 64), 64), :]

    def yblock(st, b, dy):
        yy = lax.rem(y + NY + dy, NY)
        return bufs[st].at[pl.ds(pl.multiple_of(32 * (NY * b + yy), 32), 32), :]

    def steps(st, way):
        return UP[st] if way == 0 else 15 - UP[st]

    def origin(way, s):
        return lax.rem(z + NZ - s, NZ) if way == 0 else lax.rem(z + s, NZ)

    def zpass(st, d):
        near, jump = SKIP[st]
        for way in (0, 1):
            last = steps(st, way)
            ref = zblock(st, origin(way, d))
            for hops in (1, jump):
                to = d + hops
                if hops == 1 and to > min(near, last) or hops > 1 and (d == 0 or not near < to <= last):
                    continue
                if d <= last:
                    rc(
                        ref, ref, ss.at[3 if st == 5 else st], zr.at[st, to - 1], dev(dz=hops if way == 0 else -hops)
                    ).start()

    def zs(st):
        zpass(st, 0)

    def zv(st, d):
        rows = 32 if STREAMS[st][0] == "zy" else 128 - LATE if st == 4 else 64
        ways = sum(d <= steps(st, way) for way in (0, 1))
        landed(bufs[st].at[0 : ways * rows, :], zr.at[st, d - 1])
        zpass(st, d)

    def slots(st, s):
        if s < 0:
            return [(0, 0, 0)]
        return [(1 + 8 * way + s, way, s + 1) for way in (0, 1) if s < steps(st, way)]

    def group(st, e):
        return 0 if st == 2 or e in EARLY else 1

    def y_start(st, slot, b, d, k):
        up = slot < 9
        if k == 2:
            ref = yblock(st, b, 0 if d >= DIRECT else -1 if up else 1)
            to = dev(dy=2 if d >= DIRECT else 1 if up else -1)
        else:
            ref = yblock(st, b, 0)
            to = dev(dy=1 - 2 * k)
        forwards = d < DIRECT and k == (0 if up else 1)
        sem = yfr.at[st, d] if forwards else ynr.at[st, group(st, d)]
        rc(ref, ref, ss.at[st], sem, to).start()

    def ys(st, e):
        for slot, way, d in slots(st, e - 1):
            for k in (0, 1, 2) if e >= DIRECT else (0, 1):
                y_start(st, slot, origin(way, d), d, k)

    def yf(st, e):
        blocks = slots(st, e - 1)
        landed(bufs[st].at[0 : 32 * len(blocks), :], yfr.at[st, e])
        for slot, way, d in blocks:
            y_start(st, slot, origin(way, d), d, 2)

    def yw(st, g):
        count = sum(
            len(slots(st, e - 1)) * (3 if e >= DIRECT else 2) for e in range(9) if group(st, e) == g
        )
        landed(bufs[st].at[0 : 32 * count, :], ynr.at[st, g])

    def ay_start(st, k):
        up = st % 2 == 0
        if k == 2:
            ref = yblock(st, z, -1 if up else 1)
            to = dev(dy=1 if up else -1)
        else:
            ref = yblock(st, z, 0)
            to = dev(dy=1 - 2 * k)
        rc(ref, ref, ss.at[st], ayr.at[st - 3, 0 if k == (0 if up else 1) else 1], to).start()

    def ay(st):
        ay_start(st, 0)
        ay_start(st, 1)

    def ayf(st):
        landed(bufs[st].at[0:32, :], ayr.at[st - 3, 0])
        ay_start(st, 2)

    def aye(st):
        landed(bufs[st].at[0:64, :], ayr.at[st - 3, 1])
        zs(st)

    ox_parts = ((1, 4, 0), (2, 2, 0), (3, 4, 256))

    def oxcopy(k):
        d, st, at = ox_parts[k]
        return rc(B3.at[own, :], bufs[st].at[own, at : at + 256], ss.at[5], oxr.at[0], dev(dx=-d))

    def xlcopy(s, way, k):
        rows = pl.ds(pl.multiple_of(128 * origin(way, s + 1), 128), LATE)
        at = 256 * k
        return rc(
            B3.at[rows, :], B4.at[rows, at : at + 256], ss.at[5 + k], xlr.at[0], dev(dx=-1 if k == 0 else 1)
        )

    def xl_send(s):
        for way in (0, 1):
            if s < steps(3, way):
                for k in (0, 1):
                    xlcopy(s, way, k).start()

    def tchunk(i, dx, cc):
        tt = lax.rem(x + NX + dx, NX) * 2 + cc
        return T.at[tt, pl.ds(256 * i, 256), :]

    def tcopy(i, k, recv):
        up = i % 2 == 0
        if k == 2:
            ref = tchunk(i, 2, c) if recv else tchunk(i, -1 if up else 1, c)
            to = dev(dx=1 if up else -1)
        else:
            ref = tchunk(i, 0 if not recv else (-1 if k == 0 else 1), c)
            to = dev(dx=1 if k == 0 else -1)
        return rc(ref, ref, tsem.at[0], xr.at[i, k], to)

    def dcopy(i, k, recv):
        ref = tchunk(i, (0, -1, 1, 2)[k], c if not recv else 1 - c)
        return rc(ref, ref, tsem.at[0], dr.at[i], partner)

    def ts(i):
        tload(i).wait()
        tcopy(i, 0, False).start()
        tcopy(i, 1, False).start()
        dcopy(i, 0, False).start()

    def tf(i):
        first = i % 2
        tcopy(i, first, True).wait_recv()
        tcopy(i, 2, False).start()
        dcopy(i, 1 + first, False).start()

    def tg(i):
        first = i % 2
        tcopy(i, 1 - first, True).wait_recv()
        dcopy(i, 2 - first, False).start()

    def th(i):
        tcopy(i, 2, True).wait_recv()
        dcopy(i, 3, False).start()

    def td(i):
        landed(T.at[0], dr.at[i])

    def norm(i, h):
        rows = slice(256 * i + 128 * h, 256 * i + 128 * h + 128)
        total = T[0, rows, :].astype(jnp.float32)
        for k in range(1, 8):
            total += T[k, rows, :].astype(jnp.float32)
        average = jnp.sum(total, axis=1, keepdims=True) * (1.0 / 2048)
        squares = None
        for k in range(8):
            centred = T[k, rows, :].astype(jnp.float32) - average
            squares = centred * centred if k == 0 else squares + centred * centred
        variance = jnp.sum(squares, axis=1, keepdims=True) * (1.0 / 2048)
        scale = lax.rsqrt(variance + 1e-05)
        for k in range(8):
            cols = slice(256 * k, 256 * k + 256)
            centred = T[k, rows, :].astype(jnp.float32) - average
            N[rows, cols] = (centred * scale * gain[:, cols]).astype(jnp.bfloat16)

    def part(i, pairs):
        rows = slice(256 * i, 256 * i + 256)
        qkv = ibc = None
        for d, e in pairs:
            one = pl.multiple_of(128 * origin(0, d), 128)
            two = pl.multiple_of(128 * origin(0 if d == 0 else 1, e), 128)
            left = jnp.concatenate([N[rows, pl.ds(one, 128)], N[rows, pl.ds(two, 128)]], axis=1)
            for buf in (B0, B1):
                right = jnp.concatenate([buf[pl.ds(one, 128), :], buf[pl.ds(two, 128), :]], axis=0)
                term = jnp.dot(left, right, preferred_element_type=jnp.float32)
                if buf is B0:
                    qkv = term if qkv is None else qkv + term
                else:
                    ibc = term if ibc is None else ibc + term
        return qkv, ibc

    def pe(i):
        rows = slice(256 * i, 256 * i + 256)
        qkv, ibc = part(i, [(d, d) for d in EARLY])
        PACC[rows, 0:256] = qkv
        PACC[rows, 256:640] = ibc

    def proj(i):
        rows = slice(256 * i, 256 * i + 256)
        qkv, ibc = part(i, [(d, d) for d in range(1, 8) if d not in EARLY] + [(0, 8)])
        qkv = (qkv + PACC[rows, 0:256]).astype(jnp.bfloat16)
        ibc = (ibc + PACC[rows, 256:640]).astype(jnp.bfloat16)
        Q[rows, :] = qkv[:, 0:128]
        KV[128 + 256 * i : 128 + 256 * i + 256, :] = qkv[:, 128:256]
        inner = ibc[:, 0:128].astype(jnp.float32)
        gate_c = ibc[:, 256:384].astype(jnp.float32)
        product = (gate_c * inner).astype(jnp.bfloat16)
        PR[16 + 256 * i : 16 + 256 * i + 256, :] = product.astype(jnp.float32)
        GB[rows, :] = ibc[:, 128:256]

    def halo(k):
        to = dev(dz=1)
        if k == 0:
            return rc(KV.at[1024:1152, :], KV.at[0:128, :], hsem.at[0], hr.at[0], to)
        return rc(PR.at[1032:1040, :], PR.at[8:16, :], hsem.at[1], hr.at[1], to)

    def bias_init():
        row = lax.broadcasted_iota(jnp.int32, (128, 512), 0)
        col = lax.broadcasted_iota(jnp.int32, (128, 512), 1)
        upper = col >= 256
        distance = 128 + row - jnp.where(upper, col - 256, col)
        head = jnp.where(upper, 1, 0) + 2 * t
        slope = jnp.exp2((head + 1).astype(jnp.float32) * (-8.0 / HEADS))
        keep = (distance >= 0) & (distance < WINDOW)
        BIAS[...] = jnp.where(keep, -slope * distance.astype(jnp.float32), -jnp.inf)

    def mix(k):
        for u in (0, 1):
            mix_half(k, u)

    def mix_half(k, u):
        q0 = pl.multiple_of(256 * lax.rem(x + k, NX) + 128 * u, 128)
        lane = lax.broadcasted_iota(jnp.int32, (256, 128), 1)
        low = lane < 64
        q = Q[pl.ds(q0, 128), :]
        kv = KV[pl.ds(q0, 256), :].astype(jnp.float32)
        vk = pltpu.roll(kv, 64, 1)
        keys = jnp.concatenate(
            [jnp.where(low, kv, 0.0), jnp.where(low, 0.0, vk)], axis=0
        ).astype(jnp.bfloat16)
        values = jnp.concatenate(
            [jnp.where(low, vk, 0.0), jnp.where(low, 0.0, kv)], axis=0
        ).astype(jnp.bfloat16)
        scores = lax.dot_general(q, keys, NT, preferred_element_type=jnp.float32)
        scores = scores * HEAD ** (-0.5) + BIAS[...]
        if u == 0:
            col = lax.broadcasted_iota(jnp.int32, (128, 512), 1)
            place = jnp.bitwise_and(col, 255) + (1024 * z + q0 - WINDOW)
            scores = jnp.where(place >= 0, scores, -jnp.inf)
        weights = []
        for g in range(2):
            part = scores[:, 256 * g : 256 * g + 256]
            sink = sinks[0, g]
            top = jnp.maximum(jnp.max(part, axis=1, keepdims=True), sink)
            raised = jnp.exp(part - top)
            below = jnp.sum(raised, axis=1, keepdims=True) + jnp.exp(sink - top)
            weights.append((raised * (1.0 / below)).astype(jnp.bfloat16))
        attended = jnp.dot(
            jnp.concatenate(weights, axis=1), values, preferred_element_type=jnp.float32
        )
        half = slice(128 * u, 128 * u + 128)
        AOUT[k, half, 0:128] = attended.astype(jnp.bfloat16)
        around = PR[pl.ds(pl.multiple_of(q0 + 8, 8), 136), :]
        tap = taps[...].astype(jnp.float32)
        filtered = (
            tap[0:1] * around[6:134] + tap[1:2] * around[7:135] + tap[2:3] * around[8:136]
        )
        gate_b = GB[pl.ds(q0, 128), :].astype(jnp.float32)
        AOUT[k, half, 128:256] = (gate_b * filtered).astype(jnp.bfloat16)

    def acopy(k, u):
        half = pl.ds(128 * u, 128)
        if k == 2:
            return rc(AOUT.at[k, half, :], RLY.at[u], asem.at[0], rr.at[u], dev(dx=1 - 2 * u))
        return rc(AOUT.at[k, half, :], AALL.at[NX - k, half, :], asem.at[0], ar.at[k - 1], dev(dx=k))

    def relay(u):
        half = pl.ds(128 * u, 128)
        return rc(RLY.at[u], AALL.at[2, half, :], asem.at[1], ar.at[1], dev(dx=1 - 2 * u))

    def out_dot(left, buf, n, at):
        right = buf[512 * n : 512 * n + 512, at : at + 256]
        return lax.dot_general(left, right, NT, preferred_element_type=jnp.float32)

    def excopy(n):
        return rc(XS.at[n], XR.at[n], es.at[0], er.at[n], partner)

    def store(n):
        cols = slice(512 * n, 512 * n + 512)
        return pltpu.make_async_copy(OUTV.at[:, cols], out.at[:, cols], osem.at[0])

    def start():
        bias_init()

    def ox():
        for k in range(3):
            oxcopy(k).start()

    def oxw():
        landed(B3.at[0:96, :], oxr.at[0])

    def xs(d):
        xl_send(d - 1)

    def xw():
        landed(B4.at[0 : 15 * LATE, :], xlr.at[0])

    def hs():
        halo(0).start()
        halo(1).start()

    def hw():
        halo(0).wait_recv()
        halo(1).wait_recv()
        PR[8:16, :] = jnp.where(z > 0, PR[8:16, :], 0.0)

    def asend(k):
        for u in (0, 1):
            acopy(k, u).start()

    def af(u):
        acopy(2, u).wait_recv()
        relay(u).start()

    def aw(k):
        landed(AALL.at[0], ar.at[k - 1])

    def f0():
        for n in range(4):
            ACC[:, 512 * n : 512 * n + 512] = out_dot(AOUT[0], B3, n, 0)

    def f1():
        for n in range(4):
            ACC[:, 512 * n : 512 * n + 512] += out_dot(AALL[1], B4, n, 0)

    def f3():
        for n in range(4):
            ACC[:, 512 * n : 512 * n + 512] += out_dot(AALL[3], B4, n, 256)

    def ft():
        rows = pl.ds(pl.multiple_of(128 * (1 - c), 128), 128)
        for n in range(4):
            total = ACC[rows, 512 * n : 512 * n + 512] + out_dot(AALL[2, rows, :], B2, n, 0)
            XS[n] = total.astype(jnp.bfloat16)
            if n >= 1:
                excopy(n - 1).start()

    def fo():
        rows = pl.ds(pl.multiple_of(128 * c, 128), 128)
        for n in range(4):
            cols = slice(512 * n, 512 * n + 512)
            ACC[rows, cols] += out_dot(AALL[2, rows, :], B2, n, 0)
            if n == 0:
                excopy(3).start()

    def comb():
        rows = pl.ds(pl.multiple_of(128 * c, 128), 128)
        for n in range(4):
            cols = slice(512 * n, 512 * n + 512)
            excopy(n).wait_recv()
            OUTV[:, cols] = (ACC[rows, cols] + XR[n].astype(jnp.float32)).astype(jnp.bfloat16)
            if n >= 1:
                store(n - 1).start()

    order = (
        (start,), (zs, 0), (ay, 3), (ox,), (zs, 1), (ts, 3), (ts, 2), (ys, 1, 0), (ayf, 3), (zv, 0, 1), (oxw,),
        (ay, 4), (zs, 2), (zv, 1, 1), (ts, 1), (aye, 3), (zs, 5), (zv, 0, 2), (tf, 3), (ys, 0, 0), (ayf, 4), (ts, 0),
        (zv, 2, 1), (ys, 1, 1), (ys, 0, 2), (zv, 1, 2), (zv, 3, 1), (ys, 1, 2), (zv, 5, 1), (yf, 1, 0), (zv, 0, 3),
        (zv, 2, 2), (ys, 2, 2), (ys, 0, 1), (tg, 1), (zv, 1, 3), (aye, 4), (tg, 3), (ys, 0, 3), (zv, 3, 2),
        (yf, 1, 2), (ys, 1, 3), (zv, 0, 4), (ys, 0, 4), (zv, 5, 2), (tg, 2), (yf, 0, 1), (zv, 1, 4), (zv, 2, 3),
        (yf, 0, 2), (ys, 1, 4), (zv, 4, 1), (tf, 0), (yf, 1, 1), (yf, 0, 0), (zv, 3, 3), (yf, 1, 3), (th, 3), (tf, 2),
        (zv, 0, 5), (tf, 1), (ys, 0, 5), (zv, 1, 5), (ys, 1, 5), (tg, 0), (zv, 5, 3), (yf, 1, 4), (yf, 0, 3),
        (yf, 0, 4), (zv, 2, 4), (yf, 0, 5), (zv, 4, 2), (zv, 0, 6), (ys, 0, 6), (zv, 3, 4), (yf, 1, 5), (zv, 1, 6),
        (ys, 1, 6), (zv, 0, 7), (ys, 0, 7), (th, 1), (td, 3), (zv, 5, 4), (th, 0), (yf, 0, 6), (th, 2), (xs, 4),
        (zv, 1, 7), (ys, 1, 7), (zv, 2, 5), (norm, 3, 1), (td, 1), (zv, 4, 3), (yw, 0, 0), (zv, 0, 8), (ys, 0, 8),
        (xs, 1), (td, 0), (zv, 3, 5), (norm, 3, 0), (zv, 1, 8), (ys, 1, 8), (yw, 1, 0), (zv, 5, 5), (yf, 1, 6),
        (xs, 3), (pe, 3), (norm, 0, 0), (ys, 2, 3), (xs, 2), (td, 2), (norm, 1, 0), (zv, 2, 7), (zv, 4, 4),
        (ys, 2, 7), (norm, 2, 1), (yw, 0, 1), (yf, 2, 2), (norm, 1, 1), (norm, 2, 0), (zv, 3, 6), (xs, 5), (yw, 1, 1),
        (proj, 3), (hs,), (ys, 2, 0), (yf, 2, 3), (norm, 0, 1), (pe, 1), (zv, 5, 6), (ys, 2, 1), (zv, 2, 6), (xs, 6),
        (pe, 2), (zv, 3, 7), (pe, 0), (zv, 5, 7), (zv, 4, 5), (xs, 7), (proj, 2), (proj, 0), (ys, 2, 6), (proj, 1),
        (ys, 2, 5), (hw,), (mix, 2), (asend, 2), (yf, 2, 1), (ys, 2, 4), (mix, 1), (zv, 5, 8), (zv, 2, 8), (zv, 3, 8),
        (xs, 8), (mix, 3), (yf, 2, 0), (asend, 1), (zv, 4, 6), (asend, 3), (ys, 2, 8), (yf, 2, 6), (mix, 0),
        (yf, 2, 5), (yf, 2, 4), (f0,), (af, 0), (af, 1), (yw, 2, 0), (xw,), (zv, 4, 8), (aw, 3), (zv, 4, 7), (aw, 1),
        (f1,), (f3,), (aw, 2), (ft,), (fo,), (comb,),
    )
    for event, *where in order:
        with jax.named_scope(event.__name__ + "_".join(map(str, where))):
            event(*where)
    with jax.named_scope("tail"):
        store(3).start()

    def sent(ref, sem):
        pltpu.make_async_copy(ref, ref, sem).wait()

    with jax.named_scope("sent"):
        for st in (0, 1, 2):
            sent(bufs[st].at[0:2016, :], ss.at[st])
        sent(B3.at[0:2016, :], ss.at[3])
        sent(B4.at[0 : 96 + 15 * (128 - LATE), :], ss.at[4])
        sent(B3.at[0 : 96 + 15 * LATE, :], ss.at[5])
        sent(B3.at[0 : 15 * LATE, :], ss.at[6])
        sent(T.at[0:7], tsem.at[0])
        for k in range(2):
            halo(k).wait_send()
        sent(AOUT.at[0:3], asem.at[0])
        sent(RLY, asem.at[1])
        sent(XS, es.at[0])
    with jax.named_scope("stored"):
        pltpu.make_async_copy(OUTV, out, osem.at[0]).wait()


def on_device(
    tokens, norm_gain, w_query, w_key, w_value, w_conv_in, w_conv_b, w_conv_c,
    conv_taps, sink_logits, w_attn_out, w_conv_out,
):
    hbm = pl.BlockSpec(memory_space=pl.ANY)
    bf, f32 = jnp.bfloat16, jnp.float32
    dma = pltpu.SemaphoreType.DMA
    V = pltpu.VMEM
    result = pl.pallas_call(
        kernel,
        out_shape=jax.ShapeDtypeStruct((128, 2048), bf),
        in_specs=[hbm] * 12,
        out_specs=hbm,
        scratch_shapes=[
            V((8, 1024, 256), bf), V((1024, 2048), bf),
            V((2048, 256), bf), V((2048, 384), bf), V((2048, 256), bf), V((2048, 256), bf), V((2048, 512), bf),
            V((1024, 128), bf), V((1152, 128), bf), V((1040, 128), f32), V((1024, 128), bf),
            V((128, 512), f32), V((4, 256, 256), bf), V((4, 256, 256), bf), V((2, 128, 256), bf),
            V((4, 128, 512), bf), V((4, 128, 512), bf), V((256, 2048), f32), V((128, 2048), bf), V((1024, 640), f32),
            V((1, 2048), f32), V((3, 128), bf), pltpu.SMEM((1, 2), f32), V((2, 32, 64), bf),
            dma((4,)), dma((6,)), dma((1,)),
            dma((7,)), dma((6, 8)), dma((3, max(DIRECT, 1))), dma((3, 2)), dma((2, 2)),
            dma((1,)), dma((4, 3)), dma((4,)), dma((1,)), dma((1,)),
            dma((2,)), dma((2,)), dma((2,)), dma((3,)), dma((2,)), dma((1,)), dma((4,)),
        ],
        compiler_params=pltpu.CompilerParams(
            collective_id=0, has_side_effects=True, vmem_limit_bytes=60 * 1024 * 1024
        ),
    )(
        tokens[0], norm_gain[None], w_query, w_key, w_value, w_conv_in, w_conv_b, w_conv_c,
        conv_taps, sink_logits[None], w_attn_out.T, w_conv_out.T,
    )
    return result[None]


def solution(mesh):
    placed = (
        P("fs", "sp", "tp"),
        P(),
        P(("sp", "fs"), "tp"),
        P(("sp", "fs"), "tp"),
        P(("sp", "fs"), "tp"),
        P(("sp", "fs"), "tp"),
        P(("sp", "fs"), "tp"),
        P(("sp", "fs"), "tp"),
        P(None, "tp"),
        P("tp"),
        P("tp", ("sp", "fs")),
        P("tp", ("sp", "fs")),
    )
    return jax.shard_map(
        on_device,
        mesh=mesh,
        in_specs=placed,
        out_specs=P("fs", ("sp", "tp"), None),
        check_vma=False,
    )
```
